32 devices in a mesh: sp: 4 (over y, x), tp: 8 (over z, core).
Axes of the slice: x: 2, y: 2, z: 4, core: 2. Of those that a mesh axis runs over, the one named last changes fastest.
Arguments:
- moe_input: bfloat16 [1024, 4096], P('sp', 'tp'), may hold values from -6 to 6
- out_gate: bfloat16 [1024, 4096], P('sp', 'tp'), may hold values from -6 to 6
- in_gate: bfloat16 [1024, 4096], P('sp', 'tp'), may hold values from -6 to 6
- values: bfloat16 [1024, 4096], P('sp', 'tp'), may hold values from -6 to 6
- conv_taps: float32 [3, 4096], P(None, 'tp'), may hold values from -3 to 3
- out_proj: bfloat16 [4096, 4096], P(None, 'tp'), may hold values from -0.09375 to 0.09375
- route_ids: int32 [1024, 2], P('sp'), may hold values from 0 to 3, all different within a row; in each aligned block of 256 rows (0 to 255, 256 to 511, ...) at most 192 rows name the same one
- route_gates: float32 [1024, 2], P('sp'), may hold values from 0.1 to 0.9
- expert_gate: bfloat16 [4, 4096, 2048], P('sp', None, 'tp'), may hold values from -0.09375 to 0.09375
- expert_up: bfloat16 [4, 4096, 2048], P('sp', None, 'tp'), may hold values from -0.09375 to 0.09375
- expert_down: bfloat16 [4, 2048, 4096], P('sp', 'tp'), may hold values from -0.125 to 0.125
- cotangent: bfloat16 [1024, 4096], P('sp', 'tp'), may hold values from -6 to 6
Outputs:
- grad_out_gate: bfloat16 [1024, 4096], P('sp', 'tp')
- grad_in_gate: bfloat16 [1024, 4096], P('sp', 'tp')
- grad_values: bfloat16 [1024, 4096], P('sp', 'tp')
- grad_out_proj: float32 [4096, 4096], P('sp', 'tp')
- grad_expert_gate: float32 [4, 4096, 2048], P('sp', None, 'tp')
- grad_expert_up: float32 [4, 4096, 2048], P('sp', None, 'tp')
- grad_expert_down: float32 [4, 2048, 4096], P('sp', 'tp')
The draws below stay inside these ranges and needn't reach their ends.
Inputs may be any that keep to these rules, and one draw needn't show every extreme that they name: `route_ids`: the 2 experts of a token differ. In the rows of one device no expert is named by more than 192 assignments, and in some device's rows some expert is named by exactly 192.
All inputs are finite; a program needn't handle non-finite values.
Results may differ from the reference program's by a relative error of at most 0.014.
Values may be sent and summed in bfloat16 or wider, within the bound.
A program may use at most 128 MiB of HBM per device.

```python
import math
import jax
import jax.numpy as jnp
import numpy as np
from jax import lax

D = 4096
C = 4096
F = 2048
TOP = 2
TOK = 256
EXPERTS = 4
CAP = 192
TOKENS = 1024
N_SP = 4


def strengthened(drawn, rng, source, target, blocks, factor):
    def block_of(dim):
        return (jnp.arange(drawn.shape[dim]) // (drawn.shape[dim] // blocks)).reshape((-1,) + (1,) * (drawn.ndim - 1 - dim))

    one_side = jax.random.permutation(rng, blocks)[block_of(target)]
    far = (block_of(target) + blocks // 2) % blocks
    return jnp.where((block_of(source) == one_side) | (block_of(source) == far), factor * drawn, drawn)


def steps_of(stream_key, shape, pieces, low, high):
    gain = 1.0
    for dim, parts in pieces:
        steps = jax.random.uniform(jax.random.fold_in(jax.random.fold_in(stream_key, 6), dim), (parts,), jnp.float32, low / len(pieces), high / len(pieces))
        gain = gain * jnp.repeat(jnp.exp(steps), shape[dim] // parts).reshape((-1,) + (1,) * (len(shape) - 1 - dim))
    return gain


def deal_out(key, own, number, rows, number_of, top, bound, slope):
    order = jax.random.permutation(key, number_of)
    crowded, common = load_shares(number_of, rows * top, bound, slope, True), load_shares(number_of, rows * top, bound, slope, False)
    places = jnp.arange(number_of)

    def named(sizes, turn):
        used = int((sizes > 0).sum())
        fixed = max(1, used // 4)
        moved = fixed + (places - fixed + turn * (used - fixed)) % max(1, number_of - fixed)
        return jnp.zeros((number_of,), jnp.int32).at[order[jnp.where(places < fixed, places, moved)]].set(jnp.asarray(sizes, jnp.int32))

    sizes = jnp.where(number % 4 == 0, named(crowded, number // 4), named(common, number - number // 4 - 1))
    mixed = jax.random.permutation(jax.random.fold_in(own, 3), number_of)
    source_of, receiver = mixed[0:number_of // 2 * 2:2], mixed[1:number_of // 2 * 2:2]
    margin = jnp.minimum(sizes[source_of] - 1, bound - sizes[receiver]) // 2
    margin = jnp.where((source_of == order[0]) | (receiver == order[0]) | (sizes[receiver] == 0), 0, jnp.maximum(margin, 0))
    moved = jax.random.randint(jax.random.fold_in(own, 4), (number_of // 2,), 0, 1 << 20) % (margin + 1)
    sizes = sizes.at[source_of].add(-moved).at[receiver].add(moved)
    items = jnp.searchsorted(jnp.cumsum(sizes), jnp.arange(rows * top), side="right").astype(jnp.int32)
    table = items.reshape(top, rows).T
    table = table[jax.random.permutation(jax.random.fold_in(own, 1), rows)]
    turn = jax.random.randint(jax.random.fold_in(own, 2), (rows, 1), 0, top)
    return jnp.take_along_axis(table, (jnp.arange(top)[None, :] + turn) % top, axis=1)


def load_shares(amount, total, bound, skew, full):
    loads = [(1 << 20) // math.isqrt(standing ** skew) + 1 for standing in range(1, amount + 1)]
    largest = bound if full else min(bound, max(-(-total // amount), total * loads[0] // sum(loads)))
    least = 1 if total - largest >= amount - 1 else 0
    holding, rest = [largest] + [least] * (amount - 1), total - largest - least * (amount - 1)
    while rest > 0:
        free = [i for i in range(1, amount) if holding[i] < largest] or [i for i in range(1, amount) if holding[i] < bound]
        whole, remaining = sum([loads[i] for i in free]), rest
        for i in free:
            addition = min(bound - holding[i], max(1, remaining * loads[i] // whole), rest)
            holding[i] = holding[i] + addition
            rest = rest - addition
    return np.array(holding)


def bell_draw(stream_key, shape, spread, most, cuts=(), kind=jnp.bfloat16):
    entries = spread * jax.random.normal(stream_key, shape, jnp.float32)
    if cuts:
        entries = entries * steps_of(stream_key, shape, cuts, -0.22, 0.18)
    return jnp.clip(entries, -most, most).astype(kind)


def gaussian_with(own_key, shape, scale, bound, split, heavy, kind=jnp.bfloat16):
    result = scale * jax.random.normal(own_key, shape, jnp.float32)
    if split:
        result = result * steps_of(own_key, shape, split, -0.22, 0.18)
    return jnp.clip(strengthened(result, jax.random.fold_in(own_key, 3), *heavy), -bound, bound).astype(kind)


def setup_inputs(seed: int = 0) -> dict:
    key_list = jax.random.split(jax.random.key(seed), 13)
    moe_input = bell_draw(key_list[0], (TOKENS, D), 1.0, 6.0, ((0, 4), (1, 8)))
    out_gate = bell_draw(key_list[1], (TOKENS, C), 1.0, 6.0, ((0, 4), (1, 8)))
    in_gate = bell_draw(key_list[2], (TOKENS, C), 1.0, 6.0, ((0, 4), (1, 8)))
    values = bell_draw(key_list[3], (TOKENS, C), 1.0, 6.0, ((0, 4), (1, 8)))
    conv_taps = bell_draw(key_list[4], (3, C), 0.5, 3.0, ((1, 8),), jnp.float32)
    out_proj = bell_draw(key_list[5], (D, C), C ** -0.5, 0.09375, ((1, 8),))
    route_ids_keys = jax.random.split(jax.random.fold_in(key_list[6], 1), TOKENS // TOK)
    route_ids_turns = jax.random.permutation(jax.random.fold_in(key_list[6], 3), TOKENS // TOK)
    route_ids = jax.vmap(lambda own, number: deal_out(jax.random.fold_in(key_list[6], 2), own, number, TOK, EXPERTS, TOP, CAP, 1))(route_ids_keys, route_ids_turns).reshape((TOKENS, TOP))
    route_gates = jnp.clip(0.1 + 0.79999997 * jax.random.uniform(key_list[7], (TOKENS, TOP), jnp.float32) ** steps_of(key_list[7], (TOKENS, TOP), ((0, 4),), -0.2, 0.2), 0.1, 0.9)
    expert_gate = bell_draw(key_list[8], (EXPERTS, D, F), D ** -0.5, 0.09375, ((0, 4), (2, 8)))
    expert_up = bell_draw(key_list[9], (EXPERTS, D, F), D ** -0.5, 0.09375, ((0, 4), (2, 8)))
    expert_down = bell_draw(key_list[10], (EXPERTS, F, D), F ** -0.5, 0.125, ((0, 4), (1, 8)))
    cotangent = gaussian_with(key_list[11], (TOKENS, D), 1.0, 6.0, ((0, 4), (1, 8)), (0, 1, 8, 2.0))
    return {"moe_input": moe_input, "out_gate": out_gate, "in_gate": in_gate, "values": values, "conv_taps": conv_taps, "out_proj": out_proj, "route_ids": route_ids, "route_gates": route_gates, "expert_gate": expert_gate, "expert_up": expert_up, "expert_down": expert_down, "cotangent": cotangent}


def reference(moe_input, out_gate, in_gate, values, conv_taps, out_proj, route_ids, route_gates, expert_gate, expert_up, expert_down, cotangent):
    slots = N_SP * CAP
    flat_ids = route_ids.reshape(-1)
    owner = jnp.arange(TOKENS * TOP, dtype=jnp.int32) // TOP
    one_hot = (flat_ids[:, None] == jnp.arange(EXPERTS, dtype=jnp.int32)[None, :]).astype(jnp.int32)
    blocked = one_hot.reshape(N_SP, TOK * TOP, EXPERTS)
    earlier = (jnp.cumsum(blocked, axis=1) - blocked).reshape(TOKENS * TOP, EXPERTS)
    position = jnp.sum(earlier * one_hot, axis=1).astype(jnp.int32)
    slot_index = (flat_ids * slots + (owner // TOK) * CAP + position).astype(jnp.int32)
    slot_token = jnp.full((EXPERTS * slots,), TOKENS, jnp.int32).at[slot_index].set(owner)
    slot_weight = jnp.zeros((EXPERTS * slots,), jnp.float32).at[slot_index].set(route_gates.reshape(-1))
    padded_input = jnp.concatenate([moe_input, jnp.zeros((1, D), moe_input.dtype)], axis=0)
    padded_cot = jnp.concatenate([cotangent, jnp.zeros((1, D), cotangent.dtype)], axis=0)
    contract_rows = (((0,), (0,)), ((), ()))
    contract_cols = (((1,), (1,)), ((), ()))

    def expert_backward(args):
        tokens_of, weights_of, gate_w, up_w, down_w = args
        rows = padded_input[tokens_of]
        routed = (weights_of[:, None] * padded_cot[tokens_of].astype(jnp.float32)).astype(jnp.bfloat16)
        pre_gate = jnp.dot(rows, gate_w, preferred_element_type=jnp.float32)
        pre_up = jnp.dot(rows, up_w, preferred_element_type=jnp.float32)
        gate_sig = jax.nn.sigmoid(pre_gate)
        activated = pre_gate * gate_sig
        hidden_act = (activated * pre_up).astype(jnp.bfloat16)
        grad_down = lax.dot_general(hidden_act, routed, contract_rows, preferred_element_type=jnp.float32)
        grad_hidden = lax.dot_general(routed, down_w, contract_cols, preferred_element_type=jnp.float32)
        grad_pre_gate = (grad_hidden * pre_up * gate_sig * (1.0 + pre_gate * (1.0 - gate_sig))).astype(jnp.bfloat16)
        grad_pre_up = (grad_hidden * activated).astype(jnp.bfloat16)
        grad_gate = lax.dot_general(rows, grad_pre_gate, contract_rows, preferred_element_type=jnp.float32)
        grad_up = lax.dot_general(rows, grad_pre_up, contract_rows, preferred_element_type=jnp.float32)
        assign = (lax.dot_general(grad_pre_gate, gate_w, contract_cols, preferred_element_type=jnp.float32)
                  + lax.dot_general(grad_pre_up, up_w, contract_cols, preferred_element_type=jnp.float32))
        return grad_gate, grad_up, grad_down, assign

    grad_expert_gate, grad_expert_up, grad_expert_down, assign = lax.map(
        expert_backward,
        (slot_token.reshape(EXPERTS, slots), slot_weight.reshape(EXPERTS, slots), expert_gate, expert_up, expert_down))
    flat_assign = assign.reshape(EXPERTS * slots, D)
    moe_grad = jnp.sum(flat_assign[slot_index].reshape(TOKENS, TOP, D), axis=1)
    mixer_cot = (cotangent.astype(jnp.float32) + moe_grad).astype(jnp.bfloat16)

    conv_in = in_gate.astype(jnp.float32) * values.astype(jnp.float32)
    rimmed = jnp.pad(conv_in, ((1, 1), (0, 0)))
    conv_out = rimmed[:-2] * conv_taps[0] + rimmed[1:-1] * conv_taps[1] + rimmed[2:] * conv_taps[2]
    mixed = (out_gate.astype(jnp.float32) * conv_out).astype(jnp.bfloat16)
    grad_mixed = jnp.dot(mixer_cot, out_proj, preferred_element_type=jnp.float32)
    grad_out_gate = (grad_mixed * conv_out).astype(jnp.bfloat16)
    grad_conv_out = grad_mixed * out_gate.astype(jnp.float32)
    rim_grad = jnp.pad(grad_conv_out, ((1, 1), (0, 0)))
    grad_conv_in = rim_grad[2:] * conv_taps[0] + rim_grad[1:-1] * conv_taps[1] + rim_grad[:-2] * conv_taps[2]
    grad_in_gate = (grad_conv_in * values.astype(jnp.float32)).astype(jnp.bfloat16)
    grad_values = (grad_conv_in * in_gate.astype(jnp.float32)).astype(jnp.bfloat16)
    grad_out_proj = lax.dot_general(mixer_cot, mixed, contract_rows, preferred_element_type=jnp.float32)
    return (grad_out_gate, grad_in_gate, grad_values, grad_out_proj, grad_expert_gate, grad_expert_up, grad_expert_down)
```

```python
import jax
import jax.numpy as jnp
from jax import lax
from jax.experimental import pallas as pl
from jax.experimental.pallas import tpu as pltpu
from jax.sharding import PartitionSpec as P

MESH = pl.DeviceIdType.MESH


def peers_of(group):
    sp, tp = (lax.axis_index("sp"), lax.axis_index("tp"))
    if group == "core":
        me, size = (lax.rem(tp, 2), 2)
    elif group == "z":
        me, size = (lax.div(tp, 2), lax.axis_size("tp") // 2)
    else:
        me, size = (sp, lax.axis_size("sp"))
    others = []
    for k in range(1, size):
        place = lax.rem(me + k, size)
        if group == "core":
            others.append((place, (sp, tp - me + place)))
        elif group == "z":
            others.append((place, (sp, place * 2 + lax.rem(tp, 2))))
        else:
            others.append((place, (place, tp)))
    return me, others


def group_size(group):
    if group == "core":
        return 2
    return lax.axis_size("tp") // 2 if group == "z" else lax.axis_size("sp")


def block(ref, place, width):
    return ref.at[:, pl.ds(pl.multiple_of(place * width, width), width)]


def exchange(collective_id, *ops):
    arrays = [op[2] for op in ops]
    shapes = []
    counts = []
    for kind, group, array, *rest in ops:
        size = group_size(group)
        if kind == "cores":
            shape, count = ((array.shape[0], array.shape[1] // 2), array.shape[1] // rest[0] // 2)
        elif kind == "columns":
            shape = (size - 1, array.shape[0], array.shape[1] // size)
            count = size - 1
        elif kind == "rows":
            shape, count = ((size - 1,) + array.shape[1:], size - 1)
        elif kind == "gather":
            shape, count = ((array.shape[0], array.shape[1] * size), size - 1)
        elif kind == "send":
            shape, count = (array.shape, size - 1)
        elif kind == "stack":
            shape, count = ((size,) + array.shape, size - 1)
        else:
            shape, count = (array.shape, 1)
        shapes.append(jax.ShapeDtypeStruct(shape, array.dtype))
        counts.append(count)
    total = sum(counts)

    def kernel(*refs):
        n = len(ops)
        sources, targets = (refs[:n], refs[n : 2 * n])
        send_sem, recv_sem, own_sem = refs[2 * n :]
        barrier = pltpu.get_barrier_semaphore()
        greeted = 0
        for group in sorted({op[1] for op in ops}):
            for _, device in peers_of(group)[1]:
                pl.semaphore_signal(barrier, inc=1, device_id=device, device_id_type=MESH)
                greeted += 1
        pl.semaphore_wait(barrier, greeted)
        copies = []
        local = []
        for i, (kind, group, array, *rest) in enumerate(ops):
            me, others = peers_of(group)
            source, target = (sources[i], targets[i])
            moves = []
            if kind == "cores":
                width = rest[0]
                place, device = others[0]
                for b in range(counts[i]):
                    moves.append(
                        (
                            block(source, 2 * b + place, width),
                            target.at[:, pl.ds(b * width, width)],
                            device,
                        )
                    )
            for k, (place, device) in enumerate(others):
                if kind == "columns":
                    moves.append((block(source, place, shapes[i].shape[2]), target.at[k], device))
                elif kind == "rows":
                    moves.append((source.at[place], target.at[k], device))
                elif kind == "gather":
                    moves.append((source, block(target, me, array.shape[1]), device))
                elif kind == "send":
                    moves.append((source.at[place], target.at[me], device))
                elif kind == "stack":
                    moves.append((source, target.at[me], device))
                elif kind == "swap":
                    moves.append((source, target, device))
            for a, b, device in moves:
                j = len(copies)
                copy = pltpu.make_async_remote_copy(
                    src_ref=a,
                    dst_ref=b,
                    send_sem=send_sem.at[j],
                    recv_sem=recv_sem.at[j],
                    device_id=device,
                    device_id_type=MESH,
                )
                copy.start()
                copies.append(copy)
            if kind == "gather":
                local.append((source, block(target, me, array.shape[1]), i))
            elif kind == "send":
                local.append((source.at[me], target.at[me], i))
            elif kind == "stack":
                local.append((source, target.at[me], i))
        own = [pltpu.make_async_copy(a, b, own_sem.at[i]) for a, b, i in local]
        for copy in own:
            copy.start()
        for copy in own + copies:
            copy.wait()

    return pl.pallas_call(
        kernel,
        out_shape=shapes,
        in_specs=[pl.BlockSpec(memory_space=pl.ANY)] * len(ops),
        out_specs=[pl.BlockSpec(memory_space=pl.ANY)] * len(ops),
        scratch_shapes=[
            pltpu.SemaphoreType.DMA((total,)),
            pltpu.SemaphoreType.DMA((total,)),
            pltpu.SemaphoreType.DMA((len(ops),)),
        ],
        compiler_params=pltpu.CompilerParams(collective_id=collective_id, has_side_effects=True),
    )(*arrays)


def halves(array, width):
    core = lax.rem(lax.axis_index("tp"), 2)
    blocks = [
        lax.dynamic_slice_in_dim(array, (start + core) * width, width, axis=1)
        for start in range(0, array.shape[1] // width, 2)
    ]
    return jnp.concatenate(blocks, axis=1)


def interleave(own, other, width):
    core = lax.rem(lax.axis_index("tp"), 2)
    first, second = (jnp.where(core == 0, own, other), jnp.where(core == 0, other, own))
    blocks = []
    for start in range(0, own.shape[1], width):
        blocks.append(first[:, start : start + width])
        blocks.append(second[:, start : start + width])
    return jnp.concatenate(blocks, axis=1)


def padded(array, sides, width):
    for axis, dim in sides:
        size, length = (lax.axis_size(axis), array.shape[dim])
        up = [(i, (i + 1) % size) for i in range(size - 1)]
        down = [(j, i) for i, j in up]
        last = lax.slice_in_dim(array, length - width, length, axis=dim)
        initial = lax.slice_in_dim(array, 0, width, axis=dim)
        before = lax.ppermute(last, axis, up)
        after = lax.ppermute(initial, axis, down)
        array = jnp.concatenate([before, array, after], axis=dim)
    return array


def body(
    moe_input,
    out_gate,
    in_gate,
    values,
    conv_taps,
    out_proj,
    route_ids,
    route_gates,
    expert_gate,
    expert_up,
    expert_down,
    cotangent,
):
    token_count = moe_input.shape[0]
    part_width = moe_input.shape[1]
    pick_count = route_ids.shape[1]
    group_count = lax.axis_size("sp")
    local_count = expert_gate.shape[0]
    expert_count = group_count * local_count
    capacity = 3 * token_count // expert_count
    contract_rows = (((0,), (0,)), ((), ()))
    flat_ids = route_ids.reshape(-1)
    one_hot = (flat_ids[:, None] == jnp.arange(expert_count, dtype=jnp.int32)[None, :]).astype(
        jnp.int32
    )
    earlier = jnp.cumsum(one_hot, axis=0) - one_hot
    position = jnp.sum(earlier * one_hot, axis=1)
    slot_index = flat_ids * capacity + position
    block_rows = local_count * capacity
    slots = jnp.arange(expert_count * capacity, dtype=jnp.int32)
    hits = slots[:, None, None] == slot_index.reshape(token_count, pick_count)[None, :, :]
    take = jnp.any(hits, axis=2).astype(jnp.bfloat16)
    slot_weight = jnp.sum(jnp.where(hits, route_gates[None, :, :], 0.0), axis=(1, 2))
    conv_in = in_gate.astype(jnp.float32) * values.astype(jnp.float32)
    rimmed = padded(conv_in, (("sp", 0),), 1)
    conv_out = rimmed[:-2] * conv_taps[0] + rimmed[1:-1] * conv_taps[1] + rimmed[2:] * conv_taps[2]
    mixed = (out_gate.astype(jnp.float32) * conv_out).astype(jnp.bfloat16)
    rows_z, mixed_all = exchange(4, ("gather", "z", moe_input), ("stack", "sp", mixed))
    half = rows_z.shape[1]
    send_rows = jnp.dot(take, rows_z, preferred_element_type=jnp.float32).astype(jnp.bfloat16)
    cot_z, recv_rows = exchange(
        5,
        ("gather", "z", cotangent),
        ("send", "sp", send_rows.reshape(group_count, block_rows, half)),
    )
    send_cot = (
        slot_weight[:, None] * jnp.dot(take, cot_z, preferred_element_type=jnp.float32)
    ).astype(jnp.bfloat16)
    recv_rows = recv_rows.reshape(group_count * block_rows, half)
    recv_cot, swap_rows = exchange(
        6,
        ("send", "sp", send_cot.reshape(group_count, block_rows, half)),
        ("swap", "core", recv_rows),
    )
    recv_cot = recv_cot.reshape(group_count * block_rows, half)
    (swap_cot,) = exchange(7, ("swap", "core", recv_cot))

    def by_expert(own, other):
        full = interleave(own, other, part_width)
        full = full.reshape(group_count, local_count, capacity, 2 * half)
        return jnp.swapaxes(full, 0, 1).reshape(local_count, group_count * capacity, 2 * half)

    full_rows = by_expert(recv_rows, swap_rows)
    full_cot = by_expert(recv_cot, swap_cot)
    pre_gate = jnp.einsum(
        "prd,pdf->prf", full_rows, expert_gate, preferred_element_type=jnp.float32
    )
    pre_up = jnp.einsum("prd,pdf->prf", full_rows, expert_up, preferred_element_type=jnp.float32)
    gate_sig = jax.nn.sigmoid(pre_gate)
    activated = pre_gate * gate_sig
    hidden_act = (activated * pre_up).astype(jnp.bfloat16)
    grad_expert_down = jnp.einsum(
        "prf,prd->pfd", hidden_act, full_cot, preferred_element_type=jnp.float32
    )
    grad_hidden = jnp.einsum(
        "prd,pfd->prf", full_cot, expert_down, preferred_element_type=jnp.float32
    )
    grad_pre_gate = (grad_hidden * pre_up * gate_sig * (1.0 + pre_gate * (1.0 - gate_sig))).astype(
        jnp.bfloat16
    )
    grad_pre_up = (grad_hidden * activated).astype(jnp.bfloat16)
    grad_expert_gate = jnp.einsum(
        "prd,prf->pdf", full_rows, grad_pre_gate, preferred_element_type=jnp.float32
    )
    grad_expert_up = jnp.einsum(
        "prd,prf->pdf", full_rows, grad_pre_up, preferred_element_type=jnp.float32
    )
    partial_grad = jnp.einsum(
        "prf,pdf->prd", grad_pre_gate, expert_gate, preferred_element_type=jnp.float32
    ) + jnp.einsum("prf,pdf->prd", grad_pre_up, expert_up, preferred_element_type=jnp.float32)
    me = lax.axis_index("sp")
    partial_rows = partial_grad.astype(jnp.bfloat16).reshape(local_count * group_count * capacity, -1)
    (other_core,) = exchange(1, ("cores", "core", partial_rows, part_width))
    chip_rows = (
        halves(partial_rows, part_width).astype(jnp.float32) + other_core.astype(jnp.float32)
    ).astype(jnp.bfloat16)
    chip_rows = jnp.swapaxes(
        chip_rows.reshape(local_count, group_count, capacity, half), 0, 1
    ).reshape(group_count, block_rows, half)
    (returned,) = exchange(2, ("rows", "sp", chip_rows))
    back = lax.rem(me - jnp.arange(group_count) + group_count, group_count)
    local_slots = jnp.arange(block_rows, dtype=jnp.int32)
    picks = jnp.sum(
        (slot_index.reshape(token_count, pick_count)[None, :, :, None])
        == (back[:, None] * block_rows + local_slots)[:, None, None, :],
        axis=2,
    ).astype(jnp.bfloat16)
    token_part = jnp.dot(
        picks[0],
        lax.dynamic_index_in_dim(chip_rows, me, 0, keepdims=False),
        preferred_element_type=jnp.float32,
    ) + jnp.einsum("kts,ksd->td", picks[1:], returned, preferred_element_type=jnp.float32)
    token_part = token_part.astype(jnp.bfloat16)
    (parts,) = exchange(3, ("columns", "z", token_part))
    own_part = lax.dynamic_slice_in_dim(
        token_part, lax.div(lax.axis_index("tp"), 2) * part_width, part_width, axis=1
    )
    moe_grad = own_part.astype(jnp.float32) + jnp.sum(parts.astype(jnp.float32), axis=0)
    mixer_cot = (cotangent.astype(jnp.float32) + moe_grad).astype(jnp.bfloat16)
    (mixer_z,) = exchange(8, ("gather", "z", mixer_cot))
    (mixer_other,) = exchange(9, ("swap", "core", mixer_z))
    full_mixer_cot = interleave(mixer_z, mixer_other, part_width)
    grad_mixed = jnp.dot(full_mixer_cot, out_proj, preferred_element_type=jnp.float32)
    grad_out_gate = (grad_mixed * conv_out).astype(jnp.bfloat16)
    grad_conv_out = grad_mixed * out_gate.astype(jnp.float32)
    rim_grad = padded(grad_conv_out, (("sp", 0),), 1)
    grad_conv_in = (
        rim_grad[2:] * conv_taps[0] + rim_grad[1:-1] * conv_taps[1] + rim_grad[:-2] * conv_taps[2]
    )
    grad_in_gate = (grad_conv_in * values.astype(jnp.float32)).astype(jnp.bfloat16)
    grad_values = (grad_conv_in * in_gate.astype(jnp.float32)).astype(jnp.bfloat16)
    columns = lax.all_to_all(full_mixer_cot, "sp", split_axis=1, concat_axis=0, tiled=True)
    grad_out_proj = lax.dot_general(
        columns,
        mixed_all.reshape(group_count * token_count, part_width),
        contract_rows,
        preferred_element_type=jnp.float32,
    )
    return (
        grad_out_gate,
        grad_in_gate,
        grad_values,
        grad_out_proj,
        grad_expert_gate,
        grad_expert_up,
        grad_expert_down,
    )


def flip(index, bits):
    high, low = (lax.div(index, 2), lax.rem(index, 2))
    bit_high, bit_low = (lax.div(bits, 2), lax.rem(bits, 2)) if not isinstance(bits, int) else (bits // 2, bits % 2)
    high = high + bit_high - 2 * high * bit_high
    low = low + bit_low - 2 * low * bit_low
    return 2 * high + low


def place():
    sp, tp = (lax.axis_index("sp"), lax.axis_index("tp"))
    return sp, lax.div(tp, 2), lax.rem(tp, 2)


def greet(devices):
    barrier = pltpu.get_barrier_semaphore()
    for device in devices:
        pl.semaphore_signal(barrier, inc=1, device_id=device, device_id_type=MESH)
    pl.semaphore_wait(barrier, len(devices))


def remote(source, target, send_sem, recv_sem, device):
    return pltpu.make_async_remote_copy(
        src_ref=source,
        dst_ref=target,
        send_sem=send_sem,
        recv_sem=recv_sem,
        device_id=device,
        device_id_type=MESH,
    )


def dot_nt(a, b):
    return lax.dot_general(a, b, (((1,), (1,)), ((), ())), preferred_element_type=jnp.float32)


def dot_nn(a, b):
    return jnp.dot(a, b, preferred_element_type=jnp.float32)


def experts_kernel(tokens, width, hidden):
    groups, layers = (4, 4)
    parts = 2 * layers
    rows_all = groups * tokens

    def kernel(
        x_hbm, c_hbm, route, wg_hbm, wu_hbm, wd_hbm,
        xf, cf, g_out, u_out, h_out, mixer_out,
        xc, w, wd, wp, acc, a, hb, wrow, own_sum, result,
        sd, sx, sy, sz, rd, rx, ry, rz,
        load, xc_send, xc_recv, wr_send, wr_recv, wp_send, wp_recv, a_send, a_recv,
        rs_send, rs_recv, out_sem, col_sem,
    ):
        sp, z, c = place()
        tp = 2 * z + c
        xn, yn, dn = (flip(sp, 1), flip(sp, 2), flip(sp, 3))
        near = 1 - c
        partner = (sp, 2 * z + near)
        x_dev, y_dev, d_dev = ((xn, tp), (yn, tp), (dn, tp))

        def z_dev(k):
            return (sp, 2 * flip(z, k) + c)

        def rows(s):
            return pl.ds(pl.multiple_of(s * tokens, tokens), tokens)

        def blk(t, s, part):
            return xc.at[t, part, rows(s)]

        loads = [
            pltpu.make_async_copy(x_hbm, blk(0, sp, tp), load.at[0]),
            pltpu.make_async_copy(c_hbm, blk(1, sp, tp), load.at[1]),
            pltpu.make_async_copy(wg_hbm, w.at[0], load.at[2]),
            pltpu.make_async_copy(wu_hbm, w.at[1], load.at[3]),
            pltpu.make_async_copy(route.at[sp], wrow.at[sp], load.at[4]),
        ]
        for part in range(parts):
            loads.append(
                pltpu.make_async_copy(
                    wd_hbm.at[:, pl.ds(part * width, width)], wd.at[part], load.at[5 + part]
                )
            )
        for copy in loads:
            copy.start()
        greet([partner, z_dev(1), z_dev(2), z_dev(3), x_dev, y_dev, d_dev])
        loads[0].wait()
        loads[1].wait()

        def pass_on(t, s, part, slot, device):
            return remote(
                blk(t, s, part), blk(t, s, part), xc_send.at[t, slot], xc_recv.at[t, s, part], device
            )

        def arrive(t, s, part):
            pass_on(t, s, part, 0, partner).wait_recv()

        for k in (1, 2, 3):
            for t in (0, 1):
                pass_on(t, sp, tp, 11 + k, z_dev(k)).start()
            if k == 1:
                for t in (0, 1):
                    pass_on(t, sp, tp, 4, x_dev).start()
                    pass_on(t, sp, tp, 8, y_dev).start()
                    pass_on(t, sp, tp, 0, partner).start()
        route_copies = []
        for i, (s, device) in enumerate(((xn, x_dev), (yn, y_dev), (dn, d_dev))):
            copy = remote(route.at[s], wrow.at[sp], wr_send.at[i], wr_recv.at[i], device)
            copy.start()
            route_copies.append(copy)
        for copy in loads[2:]:
            copy.wait()
        weight_copies = []
        for j in (0, 1):
            for part in range(layers):
                copy = remote(
                    w.at[j, 2 * part + near], wp.at[j, part], wp_send.at[j, part], wp_recv.at[j, part], partner
                )
                copy.start()
                weight_copies.append(copy)
        acc[...] = jnp.zeros_like(acc)

        def column_copy(t, part):
            cols = pl.ds(pl.multiple_of(part * width, width), width)
            target = (xf, cf)[t]
            return pltpu.make_async_copy(xc.at[t, part], target.at[:, cols], col_sem.at[t, part])

        def multiply(t, part):
            @pl.when(t == 0)
            def _():
                column_copy(0, part).start()

                @pl.loop(0, groups)
                def _(s):
                    tile = xc[0, part, rows(s), :]
                    acc[0, rows(s), :] += dot_nn(tile, w[0, part])
                    acc[1, rows(s), :] += dot_nn(tile, w[1, part])

            @pl.when(t == 1)
            def _():
                column_copy(1, part).start()

                @pl.loop(0, groups)
                def _(s):
                    acc[2, rows(s), :] += dot_nt(xc[1, part, rows(s), :], wd[part])

        def step(i, carry):
            r, t = (lax.div(i, 2), lax.rem(i, 2))

            @pl.when(i < 6)
            def _():
                part = 2 * flip(z, r + 1) + c
                arrive(t, sp, part)
                pass_on(t, sp, part, 5 + r, x_dev).start()
                pass_on(t, sp, part, 9 + r, y_dev).start()
                pass_on(t, sp, part, 1 + r, partner).start()

            @pl.when(i < 8)
            def _():
                part = 2 * flip(z, r) + c
                even = lax.rem(r, 2) == 0
                arrive(t, xn, part)

                @pl.when(even)
                def _():
                    pass_on(t, xn, part, 27 + r, y_dev).start()

                pass_on(t, xn, part, 15 + r, partner).start()
                arrive(t, yn, part)

                @pl.when(lax.rem(r, 2) == 1)
                def _():
                    pass_on(t, yn, part, 27 + r, x_dev).start()

                pass_on(t, yn, part, 19 + r, partner).start()

            @pl.when((i >= 2) & (i < 10))
            def _():
                part = 2 * flip(z, r - 1) + c
                arrive(t, dn, part)
                pass_on(t, dn, part, 22 + r, partner).start()

            @pl.when(i >= 3)
            def _():
                j = i - 3
                kj, tj = (lax.div(j, 2), lax.rem(j, 2))
                layer = flip(z, kj)
                multiply(tj, 2 * layer + c)
                for s in range(groups):
                    arrive(tj, s, 2 * layer + near)
                multiply(tj, 2 * layer + near)

            return carry

        lax.fori_loop(0, 11, step, 0)

        for copy in route_copies:
            copy.wait()
        for copy in weight_copies:
            copy.wait()
        half = 128
        eye = lax.broadcasted_iota(jnp.int32, (half, half), 0) == lax.broadcasted_iota(
            jnp.int32, (half, half), 1
        )
        a_copies = []
        for i, s in enumerate((dn, xn, yn, sp)):
            columns = []
            for h in range(tokens // half):
                line = jnp.broadcast_to(wrow[s, 0:1, h * half : (h + 1) * half], (half, half))
                columns.append(jnp.sum(jnp.where(eye, line, 0.0), axis=1, keepdims=True))

            for h in range(tokens // half):
                here = pl.ds(pl.multiple_of(s * tokens + h * half, half), half)
                gate, up = (acc[0, here, :], acc[1, here, :])
                back = acc[2, here, :] * columns[h]
                sig = jax.nn.sigmoid(gate)
                act = gate * sig
                hb[here, :] = (act * up * columns[h]).astype(jnp.bfloat16)
                a[0, here, :] = (back * up * sig * (1.0 + gate * (1.0 - sig))).astype(jnp.bfloat16)
                a[1, here, :] = (back * act).astype(jnp.bfloat16)
            for j in (0, 1):
                copy = remote(
                    a.at[j, rows(s)], a.at[2 + j, rows(s)], a_send.at[j, i], a_recv.at[j, i], partner
                )
                copy.start()
                a_copies.append(copy)
        outs = [
            pltpu.make_async_copy(a.at[0], g_out, out_sem.at[0]),
            pltpu.make_async_copy(a.at[1], u_out, out_sem.at[1]),
            pltpu.make_async_copy(hb, h_out, out_sem.at[2]),
        ]
        for copy in outs:
            copy.start()

        def partial(s, k, finish):
            layer = flip(z, k)
            part = 2 * layer + c
            tile = 256

            @pl.loop(0, width // tile)
            def _(n):
                cols = pl.ds(pl.multiple_of(n * tile, tile), tile)
                value = dot_nt(a[0, rows(s), :], w[0, part, cols, :])
                value += dot_nt(a[1, rows(s), :], w[1, part, cols, :])
                value += dot_nt(a[2, rows(s), :], wp[0, layer, cols, :])
                value += dot_nt(a[3, rows(s), :], wp[1, layer, cols, :])
                finish(cols, value)

        rs_copies = []

        def ship(kind, k, source, target, device):
            copy = remote(source.at[k], target.at[k], rs_send.at[kind, k], rs_recv.at[kind, k], device)
            copy.start()
            rs_copies.append(copy)
            return copy

        def landed(kind, k, source, target):
            remote(source.at[k], target.at[k], rs_send.at[kind, k], rs_recv.at[kind, k], partner).wait_recv()

        def store_in(buffer, k):
            def finish(cols, value):
                buffer[k, :, cols] = value.astype(jnp.bfloat16)

            return finish

        def merge_in(buffer, other, k):
            def finish(cols, value):
                buffer[k, :, cols] = (value + other[k, :, cols].astype(jnp.float32)).astype(jnp.bfloat16)

            return finish

        def far(even, odd):
            partial(dn, even, store_in(sd, even))
            ship(0, even, sd, rd, x_dev)
            partial(dn, odd, store_in(sd, odd))
            ship(0, odd, sd, rd, y_dev)

        def direct(even, odd):
            partial(xn, even, store_in(sx, even))
            ship(1, even, sx, rx, x_dev)
            partial(yn, odd, store_in(sy, odd))
            ship(2, odd, sy, ry, y_dev)

        def merged(even, odd):
            landed(0, even, sd, rd)
            partial(yn, even, merge_in(sy, rd, even))
            ship(2, even, sy, ry, y_dev)
            landed(0, odd, sd, rd)
            partial(xn, odd, merge_in(sx, rd, odd))
            ship(1, odd, sx, rx, x_dev)

        def collect(k):
            landed(1, k, sx, rx)
            landed(2, k, sy, ry)

            def finish(cols, value):
                total = value + rx[k, :, cols].astype(jnp.float32) + ry[k, :, cols].astype(jnp.float32)
                if k:
                    sz[k, :, cols] = total.astype(jnp.bfloat16)
                else:
                    own_sum[:, cols] = total

            partial(sp, k, finish)
            if k:
                ship(3, k, sz, rz, z_dev(k))

        for i in range(2):
            for j in (0, 1):
                a_copies[2 * i + j].wait_recv()
            if i == 0:
                far(2, 3)
        for copy in a_copies[4:]:
            copy.wait_recv()
        direct(2, 3)
        merged(2, 3)
        far(0, 1)
        direct(0, 1)
        collect(3)
        collect(2)
        merged(0, 1)
        collect(1)
        collect(0)
        for k in (3, 2, 1):
            landed(3, k, sz, rz)

        @pl.loop(0, width // 256)
        def _(n):
            cols = pl.ds(pl.multiple_of(n * 256, 256), 256)
            total = own_sum[:, cols] + xc[1, tp, rows(sp), cols].astype(jnp.float32)
            for k in (1, 2, 3):
                total += rz[k, :, cols].astype(jnp.float32)
            result[:, cols] = total.astype(jnp.bfloat16)

        last = pltpu.make_async_copy(result, mixer_out, out_sem.at[3])
        last.start()
        for copy in rs_copies + a_copies:
            copy.wait_send()
        for t in (0, 1):

            @pl.loop(0, 31)
            def _(slot):
                pass_on(t, sp, tp, slot, partner).wait_send()

            @pl.loop(0, parts)
            def _(part):
                column_copy(t, part).wait()

        for copy in outs:
            copy.wait()
        last.wait()

    block_shape = (layers, tokens, width)
    shapes = [
        jax.ShapeDtypeStruct((rows_all, parts * width), jnp.bfloat16),
        jax.ShapeDtypeStruct((rows_all, parts * width), jnp.bfloat16),
        jax.ShapeDtypeStruct((rows_all, hidden), jnp.bfloat16),
        jax.ShapeDtypeStruct((rows_all, hidden), jnp.bfloat16),
        jax.ShapeDtypeStruct((rows_all, hidden), jnp.bfloat16),
        jax.ShapeDtypeStruct((tokens, width), jnp.bfloat16),
    ]
    half = jnp.bfloat16
    return pl.pallas_call(
        kernel,
        out_shape=shapes,
        in_specs=[pl.BlockSpec(memory_space=pl.ANY)] * 6,
        out_specs=[pl.BlockSpec(memory_space=pl.ANY)] * 6,
        scratch_shapes=[
            pltpu.VMEM((2, parts, rows_all, width), half),
            pltpu.VMEM((2, parts, width, hidden), half),
            pltpu.VMEM((parts, hidden, width), half),
            pltpu.VMEM((2, layers, width, hidden), half),
            pltpu.VMEM((3, rows_all, hidden), jnp.float32),
            pltpu.VMEM((4, rows_all, hidden), half),
            pltpu.VMEM((rows_all, hidden), half),
            pltpu.VMEM((groups, 8, tokens), jnp.float32),
            pltpu.VMEM((tokens, width), jnp.float32),
            pltpu.VMEM((tokens, width), half),
        ]
        + [pltpu.VMEM(block_shape, half)] * 8
        + [
            pltpu.SemaphoreType.DMA((5 + parts,)),
            pltpu.SemaphoreType.DMA((2, 31)),
            pltpu.SemaphoreType.DMA((2, groups, parts)),
            pltpu.SemaphoreType.DMA((3,)),
            pltpu.SemaphoreType.DMA((3,)),
            pltpu.SemaphoreType.DMA((2, layers)),
            pltpu.SemaphoreType.DMA((2, layers)),
            pltpu.SemaphoreType.DMA((2, groups)),
            pltpu.SemaphoreType.DMA((2, groups)),
            pltpu.SemaphoreType.DMA((4, layers)),
            pltpu.SemaphoreType.DMA((4, layers)),
            pltpu.SemaphoreType.DMA((4,)),
            pltpu.SemaphoreType.DMA((2, parts)),
        ],
        compiler_params=pltpu.CompilerParams(
            collective_id=10, has_side_effects=True, vmem_limit_bytes=60 * 1024 * 1024
        ),
    )


def near_body(
    moe_input,
    out_gate,
    in_gate,
    values,
    conv_taps,
    out_proj,
    route_ids,
    route_gates,
    expert_gate,
    expert_up,
    expert_down,
    cotangent,
):
    token_count, part_width = moe_input.shape
    group_count = lax.axis_size("sp")
    hidden = expert_gate.shape[2]
    part_count = lax.axis_size("tp")
    contract_rows = (((0,), (0,)), ((), ()))
    chosen = route_ids[None, :, :] == jnp.arange(group_count, dtype=jnp.int32)[:, None, None]
    weights = jnp.sum(jnp.where(chosen, route_gates[None, :, :], 0.0), axis=2)
    route = jnp.broadcast_to(weights[:, None, :], (group_count, 8, token_count))
    x_all, cot_all, grad_pre_gate, grad_pre_up, hidden_act, mixer_cot = experts_kernel(
        token_count, part_width, hidden
    )(
        moe_input,
        cotangent,
        route,
        expert_gate.reshape(part_count, part_width, hidden),
        expert_up.reshape(part_count, part_width, hidden),
        expert_down[0],
    )

    def outer(a, b):
        return lax.dot_general(a, b, contract_rows, preferred_element_type=jnp.float32)[None]

    grad_expert_gate = outer(x_all, grad_pre_gate)
    grad_expert_up = outer(x_all, grad_pre_up)
    grad_expert_down = outer(hidden_act, cot_all)
    conv_in = in_gate.astype(jnp.float32) * values.astype(jnp.float32)
    rimmed = padded(conv_in, (("sp", 0),), 1)
    conv_out = rimmed[:-2] * conv_taps[0] + rimmed[1:-1] * conv_taps[1] + rimmed[2:] * conv_taps[2]
    mixed = (out_gate.astype(jnp.float32) * conv_out).astype(jnp.bfloat16)
    mixer_z, mixed_all = exchange(8, ("gather", "z", mixer_cot), ("stack", "sp", mixed))
    (mixer_other,) = exchange(9, ("swap", "core", mixer_z))
    full_mixer_cot = interleave(mixer_z, mixer_other, part_width)
    grad_mixed = jnp.dot(full_mixer_cot, out_proj, preferred_element_type=jnp.float32)
    grad_out_gate = (grad_mixed * conv_out).astype(jnp.bfloat16)
    grad_conv_out = grad_mixed * out_gate.astype(jnp.float32)
    rim_grad = padded(grad_conv_out, (("sp", 0),), 1)
    grad_conv_in = (
        rim_grad[2:] * conv_taps[0] + rim_grad[1:-1] * conv_taps[1] + rim_grad[:-2] * conv_taps[2]
    )
    grad_in_gate = (grad_conv_in * values.astype(jnp.float32)).astype(jnp.bfloat16)
    grad_values = (grad_conv_in * in_gate.astype(jnp.float32)).astype(jnp.bfloat16)
    columns = lax.all_to_all(full_mixer_cot, "sp", split_axis=1, concat_axis=0, tiled=True)
    grad_out_proj = lax.dot_general(
        columns,
        mixed_all.reshape(group_count * token_count, part_width),
        contract_rows,
        preferred_element_type=jnp.float32,
    )
    return (
        grad_out_gate,
        grad_in_gate,
        grad_values,
        grad_out_proj,
        grad_expert_gate,
        grad_expert_up,
        grad_expert_down,
    )


def solution(mesh):
    square = mesh.shape["sp"] == 4 and mesh.shape["tp"] == 8
    return jax.shard_map(
        near_body if square else body,
        mesh=mesh,
        in_specs=(
            P("sp", "tp"),
            P("sp", "tp"),
            P("sp", "tp"),
            P("sp", "tp"),
            P(None, "tp"),
            P(None, "tp"),
            P("sp", None),
            P("sp", None),
            P("sp", None, "tp"),
            P("sp", None, "tp"),
            P("sp", "tp", None),
            P("sp", "tp"),
        ),
        out_specs=(
            P("sp", "tp"),
            P("sp", "tp"),
            P("sp", "tp"),
            P("sp", "tp"),
            P("sp", None, "tp"),
            P("sp", None, "tp"),
            P("sp", "tp", None),
        ),
        check_vma=False,
    )
```

```python
import jax
import jax.numpy as jnp
from jax import lax
from jax.experimental import pallas as pl
from jax.experimental.pallas import tpu as pltpu
from jax.sharding import PartitionSpec as P

MESH = pl.DeviceIdType.MESH


def peers_of(group):
    sp, tp = (lax.axis_index("sp"), lax.axis_index("tp"))
    if group == "core":
        me, size = (lax.rem(tp, 2), 2)
    elif group == "z":
        me, size = (lax.div(tp, 2), lax.axis_size("tp") // 2)
    else:
        me, size = (sp, lax.axis_size("sp"))
    others = []
    for k in range(1, size):
        place = lax.rem(me + k, size)
        if group == "core":
            others.append((place, (sp, tp - me + place)))
        elif group == "z":
            others.append((place, (sp, place * 2 + lax.rem(tp, 2))))
        else:
            others.append((place, (place, tp)))
    return me, others


def group_size(group):
    if group == "core":
        return 2
    return lax.axis_size("tp") // 2 if group == "z" else lax.axis_size("sp")


def block(ref, place, width):
    return ref.at[:, pl.ds(pl.multiple_of(place * width, width), width)]


def exchange(collective_id, *ops):
    arrays = [op[2] for op in ops]
    shapes = []
    counts = []
    for kind, group, array, *rest in ops:
        size = group_size(group)
        if kind == "cores":
            shape, count = ((array.shape[0], array.shape[1] // 2), array.shape[1] // rest[0] // 2)
        elif kind == "columns":
            shape = (size - 1, array.shape[0], array.shape[1] // size)
            count = size - 1
        elif kind == "rows":
            shape, count = ((size - 1,) + array.shape[1:], size - 1)
        elif kind == "gather":
            shape, count = ((array.shape[0], array.shape[1] * size), size - 1)
        elif kind == "send":
            shape, count = (array.shape, size - 1)
        elif kind == "stack":
            shape, count = ((size,) + array.shape, size - 1)
        else:
            shape, count = (array.shape, 1)
        shapes.append(jax.ShapeDtypeStruct(shape, array.dtype))
        counts.append(count)
    total = sum(counts)

    def kernel(*refs):
        n = len(ops)
        sources, targets = (refs[:n], refs[n : 2 * n])
        send_sem, recv_sem, own_sem = refs[2 * n :]
        barrier = pltpu.get_barrier_semaphore()
        greeted = 0
        for group in sorted({op[1] for op in ops}):
            for _, device in peers_of(group)[1]:
                pl.semaphore_signal(barrier, inc=1, device_id=device, device_id_type=MESH)
                greeted += 1
        pl.semaphore_wait(barrier, greeted)
        copies = []
        local = []
        for i, (kind, group, array, *rest) in enumerate(ops):
            me, others = peers_of(group)
            source, target = (sources[i], targets[i])
            moves = []
            if kind == "cores":
                width = rest[0]
                place, device = others[0]
                for b in range(counts[i]):
                    moves.append(
                        (
                            block(source, 2 * b + place, width),
                            target.at[:, pl.ds(b * width, width)],
                            device,
                        )
                    )
            for k, (place, device) in enumerate(others):
                if kind == "columns":
                    moves.append((block(source, place, shapes[i].shape[2]), target.at[k], device))
                elif kind == "rows":
                    moves.append((source.at[place], target.at[k], device))
                elif kind == "gather":
                    moves.append((source, block(target, me, array.shape[1]), device))
                elif kind == "send":
                    moves.append((source.at[place], target.at[me], device))
                elif kind == "stack":
                    moves.append((source, target.at[me], device))
                elif kind == "swap":
                    moves.append((source, target, device))
            for a, b, device in moves:
                j = len(copies)
                copy = pltpu.make_async_remote_copy(
                    src_ref=a,
                    dst_ref=b,
                    send_sem=send_sem.at[j],
                    recv_sem=recv_sem.at[j],
                    device_id=device,
                    device_id_type=MESH,
                )
                copy.start()
                copies.append(copy)
            if kind == "gather":
                local.append((source, block(target, me, array.shape[1]), i))
            elif kind == "send":
                local.append((source.at[me], target.at[me], i))
            elif kind == "stack":
                local.append((source, target.at[me], i))
        own = [pltpu.make_async_copy(a, b, own_sem.at[i]) for a, b, i in local]
        for copy in own:
            copy.start()
        for copy in own + copies:
            copy.wait()

    return pl.pallas_call(
        kernel,
        out_shape=shapes,
        in_specs=[pl.BlockSpec(memory_space=pl.ANY)] * len(ops),
        out_specs=[pl.BlockSpec(memory_space=pl.ANY)] * len(ops),
        scratch_shapes=[
            pltpu.SemaphoreType.DMA((total,)),
            pltpu.SemaphoreType.DMA((total,)),
            pltpu.SemaphoreType.DMA((len(ops),)),
        ],
        compiler_params=pltpu.CompilerParams(collective_id=collective_id, has_side_effects=True),
    )(*arrays)


def halves(array, width):
    core = lax.rem(lax.axis_index("tp"), 2)
    blocks = [
        lax.dynamic_slice_in_dim(array, (start + core) * width, width, axis=1)
        for start in range(0, array.shape[1] // width, 2)
    ]
    return jnp.concatenate(blocks, axis=1)


def interleave(own, other, width):
    core = lax.rem(lax.axis_index("tp"), 2)
    first, second = (jnp.where(core == 0, own, other), jnp.where(core == 0, other, own))
    blocks = []
    for start in range(0, own.shape[1], width):
        blocks.append(first[:, start : start + width])
        blocks.append(second[:, start : start + width])
    return jnp.concatenate(blocks, axis=1)


def padded(array, sides, width):
    for axis, dim in sides:
        size, length = (lax.axis_size(axis), array.shape[dim])
        up = [(i, (i + 1) % size) for i in range(size - 1)]
        down = [(j, i) for i, j in up]
        last = lax.slice_in_dim(array, length - width, length, axis=dim)
        initial = lax.slice_in_dim(array, 0, width, axis=dim)
        before = lax.ppermute(last, axis, up)
        after = lax.ppermute(initial, axis, down)
        array = jnp.concatenate([before, array, after], axis=dim)
    return array


def body(
    moe_input,
    out_gate,
    in_gate,
    values,
    conv_taps,
    out_proj,
    route_ids,
    route_gates,
    expert_gate,
    expert_up,
    expert_down,
    cotangent,
):
    token_count = moe_input.shape[0]
    part_width = moe_input.shape[1]
    pick_count = route_ids.shape[1]
    group_count = lax.axis_size("sp")
    local_count = expert_gate.shape[0]
    expert_count = group_count * local_count
    capacity = 3 * token_count // expert_count
    contract_rows = (((0,), (0,)), ((), ()))
    flat_ids = route_ids.reshape(-1)
    one_hot = (flat_ids[:, None] == jnp.arange(expert_count, dtype=jnp.int32)[None, :]).astype(
        jnp.int32
    )
    earlier = jnp.cumsum(one_hot, axis=0) - one_hot
    position = jnp.sum(earlier * one_hot, axis=1)
    slot_index = flat_ids * capacity + position
    block_rows = local_count * capacity
    slots = jnp.arange(expert_count * capacity, dtype=jnp.int32)
    hits = slots[:, None, None] == slot_index.reshape(token_count, pick_count)[None, :, :]
    take = jnp.any(hits, axis=2).astype(jnp.bfloat16)
    slot_weight = jnp.sum(jnp.where(hits, route_gates[None, :, :], 0.0), axis=(1, 2))
    conv_in = in_gate.astype(jnp.float32) * values.astype(jnp.float32)
    rimmed = padded(conv_in, (("sp", 0),), 1)
    conv_out = rimmed[:-2] * conv_taps[0] + rimmed[1:-1] * conv_taps[1] + rimmed[2:] * conv_taps[2]
    mixed = (out_gate.astype(jnp.float32) * conv_out).astype(jnp.bfloat16)
    rows_z, mixed_all = exchange(4, ("gather", "z", moe_input), ("stack", "sp", mixed))
    half = rows_z.shape[1]
    send_rows = jnp.dot(take, rows_z, preferred_element_type=jnp.float32).astype(jnp.bfloat16)
    cot_z, recv_rows = exchange(
        5,
        ("gather", "z", cotangent),
        ("send", "sp", send_rows.reshape(group_count, block_rows, half)),
    )
    send_cot = (
        slot_weight[:, None] * jnp.dot(take, cot_z, preferred_element_type=jnp.float32)
    ).astype(jnp.bfloat16)
    recv_rows = recv_rows.reshape(group_count * block_rows, half)
    recv_cot, swap_rows = exchange(
        6,
        ("send", "sp", send_cot.reshape(group_count, block_rows, half)),
        ("swap", "core", recv_rows),
    )
    recv_cot = recv_cot.reshape(group_count * block_rows, half)
    (swap_cot,) = exchange(7, ("swap", "core", recv_cot))

    def by_expert(own, other):
        full = interleave(own, other, part_width)
        full = full.reshape(group_count, local_count, capacity, 2 * half)
        return jnp.swapaxes(full, 0, 1).reshape(local_count, group_count * capacity, 2 * half)

    full_rows = by_expert(recv_rows, swap_rows)
    full_cot = by_expert(recv_cot, swap_cot)
    pre_gate = jnp.einsum(
        "prd,pdf->prf", full_rows, expert_gate, preferred_element_type=jnp.float32
    )
    pre_up = jnp.einsum("prd,pdf->prf", full_rows, expert_up, preferred_element_type=jnp.float32)
    gate_sig = jax.nn.sigmoid(pre_gate)
    activated = pre_gate * gate_sig
    hidden_act = (activated * pre_up).astype(jnp.bfloat16)
    grad_expert_down = jnp.einsum(
        "prf,prd->pfd", hidden_act, full_cot, preferred_element_type=jnp.float32
    )
    grad_hidden = jnp.einsum(
        "prd,pfd->prf", full_cot, expert_down, preferred_element_type=jnp.float32
    )
    grad_pre_gate = (grad_hidden * pre_up * gate_sig * (1.0 + pre_gate * (1.0 - gate_sig))).astype(
        jnp.bfloat16
    )
    grad_pre_up = (grad_hidden * activated).astype(jnp.bfloat16)
    grad_expert_gate = jnp.einsum(
        "prd,prf->pdf", full_rows, grad_pre_gate, preferred_element_type=jnp.float32
    )
    grad_expert_up = jnp.einsum(
        "prd,prf->pdf", full_rows, grad_pre_up, preferred_element_type=jnp.float32
    )
    partial_grad = jnp.einsum(
        "prf,pdf->prd", grad_pre_gate, expert_gate, preferred_element_type=jnp.float32
    ) + jnp.einsum("prf,pdf->prd", grad_pre_up, expert_up, preferred_element_type=jnp.float32)
    me = lax.axis_index("sp")
    partial_rows = partial_grad.astype(jnp.bfloat16).reshape(local_count * group_count * capacity, -1)
    (other_core,) = exchange(1, ("cores", "core", partial_rows, part_width))
    chip_rows = (
        halves(partial_rows, part_width).astype(jnp.float32) + other_core.astype(jnp.float32)
    ).astype(jnp.bfloat16)
    chip_rows = jnp.swapaxes(
        chip_rows.reshape(local_count, group_count, capacity, half), 0, 1
    ).reshape(group_count, block_rows, half)
    (returned,) = exchange(2, ("rows", "sp", chip_rows))
    back = lax.rem(me - jnp.arange(group_count) + group_count, group_count)
    local_slots = jnp.arange(block_rows, dtype=jnp.int32)
    picks = jnp.sum(
        (slot_index.reshape(token_count, pick_count)[None, :, :, None])
        == (back[:, None] * block_rows + local_slots)[:, None, None, :],
        axis=2,
    ).astype(jnp.bfloat16)
    token_part = jnp.dot(
        picks[0],
        lax.dynamic_index_in_dim(chip_rows, me, 0, keepdims=False),
        preferred_element_type=jnp.float32,
    ) + jnp.einsum("kts,ksd->td", picks[1:], returned, preferred_element_type=jnp.float32)
    token_part = token_part.astype(jnp.bfloat16)
    (parts,) = exchange(3, ("columns", "z", token_part))
    own_part = lax.dynamic_slice_in_dim(
        token_part, lax.div(lax.axis_index("tp"), 2) * part_width, part_width, axis=1
    )
    moe_grad = own_part.astype(jnp.float32) + jnp.sum(parts.astype(jnp.float32), axis=0)
    mixer_cot = (cotangent.astype(jnp.float32) + moe_grad).astype(jnp.bfloat16)
    (mixer_z,) = exchange(8, ("gather", "z", mixer_cot))
    (mixer_other,) = exchange(9, ("swap", "core", mixer_z))
    full_mixer_cot = interleave(mixer_z, mixer_other, part_width)
    grad_mixed = jnp.dot(full_mixer_cot, out_proj, preferred_element_type=jnp.float32)
    grad_out_gate = (grad_mixed * conv_out).astype(jnp.bfloat16)
    grad_conv_out = grad_mixed * out_gate.astype(jnp.float32)
    rim_grad = padded(grad_conv_out, (("sp", 0),), 1)
    grad_conv_in = (
        rim_grad[2:] * conv_taps[0] + rim_grad[1:-1] * conv_taps[1] + rim_grad[:-2] * conv_taps[2]
    )
    grad_in_gate = (grad_conv_in * values.astype(jnp.float32)).astype(jnp.bfloat16)
    grad_values = (grad_conv_in * in_gate.astype(jnp.float32)).astype(jnp.bfloat16)
    columns = lax.all_to_all(full_mixer_cot, "sp", split_axis=1, concat_axis=0, tiled=True)
    grad_out_proj = lax.dot_general(
        columns,
        mixed_all.reshape(group_count * token_count, part_width),
        contract_rows,
        preferred_element_type=jnp.float32,
    )
    return (
        grad_out_gate,
        grad_in_gate,
        grad_values,
        grad_out_proj,
        grad_expert_gate,
        grad_expert_up,
        grad_expert_down,
    )


def flip(index, bits):
    high, low = (lax.div(index, 2), lax.rem(index, 2))
    bit_high, bit_low = (lax.div(bits, 2), lax.rem(bits, 2)) if not isinstance(bits, int) else (bits // 2, bits % 2)
    high = high + bit_high - 2 * high * bit_high
    low = low + bit_low - 2 * low * bit_low
    return 2 * high + low


def place():
    sp, tp = (lax.axis_index("sp"), lax.axis_index("tp"))
    return sp, lax.div(tp, 2), lax.rem(tp, 2)


def greet(devices):
    barrier = pltpu.get_barrier_semaphore()
    for device in devices:
        pl.semaphore_signal(barrier, inc=1, device_id=device, device_id_type=MESH)
    pl.semaphore_wait(barrier, len(devices))


def remote(source, target, send_sem, recv_sem, device):
    return pltpu.make_async_remote_copy(
        src_ref=source,
        dst_ref=target,
        send_sem=send_sem,
        recv_sem=recv_sem,
        device_id=device,
        device_id_type=MESH,
    )


def dot_nt(a, b):
    return lax.dot_general(a, b, (((1,), (1,)), ((), ())), preferred_element_type=jnp.float32)


def dot_nn(a, b):
    return jnp.dot(a, b, preferred_element_type=jnp.float32)


def dot_tn(a, b):
    return lax.dot_general(a, b, (((0,), (0,)), ((), ())), preferred_element_type=jnp.float32)


def experts_kernel(tokens, width, hidden):
    groups, layers = (4, 4)
    parts = 2 * layers
    rows_all = groups * tokens

    def kernel(
        x_hbm, c_hbm, route, wg_hbm, wu_hbm, wd_hbm, og_hbm, ig_hbm, va_hbm, taps, op_hbm,
        gg_out, gu_out, gd_out, gog_out, gig_out, gva_out, gop_out,
        xc, w, wd, wp, acc, acc_down, a, a_far, ht, stage, wrow, sums,
        sd, sx, sy, sz, rd, rx, ry, rz,
        op, m, cols_in, mixed, ci, gc, conv, gm, gates, outs_v,
        load, xc_send, xc_recv, wr_send, wr_recv, wp_send, wp_recv, a_send, a_recv,
        rs_send, rs_recv, z_send, z_recv, out_sem, st_sem, gd_sem,
        edge_send, edge_recv, mx_send, mx_recv, m_send, m_recv, a2_send, a2_recv, a2p_send, a2p_recv,
    ):
        sp, z, c = place()
        tp = 2 * z + c
        xn, yn, dn = (flip(sp, 1), flip(sp, 2), flip(sp, 3))
        near = 1 - c
        partner = (sp, 2 * z + near)
        x_dev, y_dev, d_dev = ((xn, tp), (yn, tp), (dn, tp))

        mid = lax.rem(lax.div(z, 2) + lax.rem(z, 2), 2)
        inner = mid == 1

        def z_dev(k):
            return (sp, 2 * flip(z, k) + c)

        def rows(s):
            return pl.ds(pl.multiple_of(s * tokens, tokens), tokens)

        def blk(t, s, part):
            return xc.at[t, part, rows(s)]

        loads = [
            pltpu.make_async_copy(x_hbm, blk(0, sp, tp), load.at[0]),
            pltpu.make_async_copy(c_hbm, blk(1, sp, tp), load.at[1]),
            pltpu.make_async_copy(wg_hbm, w.at[:, :, pl.ds(0, hidden)], load.at[2]),
            pltpu.make_async_copy(wu_hbm, w.at[:, :, pl.ds(hidden, hidden)], load.at[3]),
            pltpu.make_async_copy(route.at[sp], wrow.at[sp], load.at[4]),
        ]
        for part in range(parts):
            loads.append(
                pltpu.make_async_copy(
                    wd_hbm.at[:, pl.ds(part * width, width)], wd.at[part], load.at[5 + part]
                )
            )
        conv_loads = [
            pltpu.make_async_copy(source, gates.at[j], load.at[5 + parts + j])
            for j, source in enumerate((og_hbm, ig_hbm, va_hbm))
        ]
        op_load = pltpu.make_async_copy(op_hbm, op, load.at[8 + parts])
        for copy in loads[:2] + conv_loads + loads[2:] + [op_load]:
            copy.start()
        pad = 8
        middle = pl.ds(pad, tokens)

        def edges(buffer, phase):
            before, after = (lax.rem(sp + groups - 1, groups), lax.rem(sp + 1, groups))
            top, low = (pl.ds(0, pad), pl.ds(pad + tokens, pad))
            first, final = (pl.ds(pad, pad), pl.ds(tokens, pad))
            return [
                remote(
                    buffer.at[final], buffer.at[top], edge_send.at[phase, 0], edge_recv.at[phase, 0], (after, tp)
                ),
                remote(
                    buffer.at[first], buffer.at[low], edge_send.at[phase, 1], edge_recv.at[phase, 1], (before, tp)
                ),
            ]

        def close_edges(buffer, copies):
            for copy in copies:
                copy.wait_recv()

            @pl.when(sp == 0)
            def _():
                buffer[pl.ds(0, pad), :] = jnp.zeros((pad, width), jnp.float32)

            @pl.when(sp == groups - 1)
            def _():
                buffer[pl.ds(pad + tokens, pad), :] = jnp.zeros((pad, width), jnp.float32)

        ci_edges = edges(ci, 0)
        greet([partner, z_dev(1), z_dev(2), z_dev(3), x_dev, y_dev, d_dev])
        loads[0].wait()
        loads[1].wait()

        def pass_on(t, s, part, slot, device):
            return remote(
                blk(t, s, part), blk(t, s, part), xc_send.at[t, slot], xc_recv.at[t, s, part], device
            )

        def arrive(t, s, part):
            pass_on(t, s, part, 0, partner).wait_recv()

        for t in (0, 1):
            pass_on(t, sp, tp, 12, z_dev(1)).start()

            @pl.when(inner)
            def _():
                pass_on(t, sp, tp, 13, z_dev(3)).start()

            pass_on(t, sp, tp, 4, x_dev).start()
            pass_on(t, sp, tp, 8, y_dev).start()
            pass_on(t, sp, tp, 0, partner).start()
        for copy in conv_loads:
            copy.wait()
        ci[middle, :] = gates[1].astype(jnp.float32) * gates[2].astype(jnp.float32)
        for copy in ci_edges:
            copy.start()
        route_copies = []
        for i, (s, device) in enumerate(((xn, x_dev), (yn, y_dev), (dn, d_dev))):
            copy = remote(route.at[s], wrow.at[sp], wr_send.at[i], wr_recv.at[i], device)
            copy.start()
            route_copies.append(copy)
        for copy in loads[2:]:
            copy.wait()
        weight_copies = []
        for part in range(layers):
            copy = remote(w.at[2 * part + near], wp.at[part], wp_send.at[part], wp_recv.at[part], partner)
            copy.start()
            weight_copies.append(copy)
        acc[...] = jnp.zeros_like(acc)
        acc_down[...] = jnp.zeros_like(acc_down)

        @pl.when(mid == 0)
        def _():
            rz[...] = jnp.zeros_like(rz)

        def multiply(t, layer):
            @pl.when(t == 0)
            def _():
                @pl.loop(0, groups)
                def _(s):
                    here = rows(s)
                    acc[here, :] += dot_nn(xc[0, 2 * layer, here, :], w[2 * layer]) + dot_nn(
                        xc[0, 2 * layer + 1, here, :], w[2 * layer + 1]
                    )

            @pl.when(t == 1)
            def _():
                @pl.loop(0, groups)
                def _(s):
                    here = rows(s)
                    acc_down[here, :] += dot_nt(xc[1, 2 * layer, here, :], wd[2 * layer]) + dot_nt(
                        xc[1, 2 * layer + 1, here, :], wd[2 * layer + 1]
                    )

        def turn(i):
            return flip(z, i + mid * lax.div(i, 2) * (5 - 2 * i))

        def step(i, carry):
            r, t = (lax.div(i, 2), lax.rem(i, 2))

            def onward(s, part, m, slot):
                @pl.when(inner & (m == 1))
                def _():
                    pass_on(t, s, part, slot, z_dev(3)).start()

                @pl.when(inner & (m > 1))
                def _():
                    pass_on(t, s, part, slot + m - 1, z_dev(1)).start()

            @pl.when(i < 6)
            def _():
                part = 2 * turn(r + 1) + c
                arrive(t, sp, part)
                onward(sp, part, r + 1, 28)
                pass_on(t, sp, part, 5 + r, x_dev).start()
                pass_on(t, sp, part, 9 + r, y_dev).start()
                pass_on(t, sp, part, 1 + r, partner).start()

            @pl.when(i < 8)
            def _():
                part = 2 * turn(r) + c
                even = lax.rem(r, 2) == 0
                arrive(t, xn, part)

                @pl.when(even & (t * r == 0))
                def _():
                    pass_on(t, xn, part, 31 + r, y_dev).start()

                pass_on(t, xn, part, 15 + r, partner).start()
                arrive(t, yn, part)

                @pl.when((lax.rem(r, 2) == 1) & (t * r == 0))
                def _():
                    pass_on(t, yn, part, 31 + r, x_dev).start()

                pass_on(t, yn, part, 19 + r, partner).start()

            @pl.when((i >= 2) & (i < 10))
            def _():
                m = r - 1
                part = 2 * turn(m) + c
                arrive(t, dn, part)

                @pl.when((t == 1) & (m == 0))
                def _():
                    pass_on(t, dn, part, 35, z_dev(1)).start()

                    @pl.when(inner)
                    def _():
                        pass_on(t, dn, part, 36, z_dev(3)).start()

                @pl.when((t == 1) & (m > 0))
                def _():
                    onward(dn, part, m, 37)

                pass_on(t, dn, part, 22 + r, partner).start()

            @pl.when(i == 2)
            def _():
                close_edges(ci, ci_edges)
                conv[...] = (
                    ci[pl.ds(pad - 1, tokens), :] * taps[0:1, :]
                    + ci[middle, :] * taps[1:2, :]
                    + ci[pl.ds(pad + 1, tokens), :] * taps[2:3, :]
                )
                mixed[sp] = (gates[0].astype(jnp.float32) * conv[...]).astype(jnp.bfloat16)

            @pl.when(i >= 3)
            def _():
                j = i - 3
                kj, tj = (lax.div(j, 2), lax.rem(j, 2))
                layer = turn(kj)
                for s in range(groups):
                    arrive(tj, s, 2 * layer + near)
                multiply(tj, layer)

            return carry

        lax.fori_loop(0, 11, step, 0)

        for copy in route_copies:
            copy.wait()
        for copy in weight_copies:
            copy.wait()
        half = 128
        eye = lax.broadcasted_iota(jnp.int32, (half, half), 0) == lax.broadcasted_iota(
            jnp.int32, (half, half), 1
        )
        a_copies = []

        def gate_rows(i, s):
            columns = []
            for h in range(tokens // half):
                line = jnp.broadcast_to(wrow[s, 0:1, h * half : (h + 1) * half], (half, half))
                columns.append(jnp.sum(jnp.where(eye, line, 0.0), axis=1, keepdims=True))

            for h in range(tokens // half):
                start = pl.multiple_of(s * tokens + h * half, half)
                here = pl.ds(start, half)
                gate, up = (acc[here, pl.ds(0, hidden)], acc[here, pl.ds(hidden, hidden)])
                back = acc_down[here, :] * columns[h]
                sig = jax.nn.sigmoid(gate)
                act = gate * sig
                a[here, pl.ds(0, hidden)] = (back * up * sig * (1.0 + gate * (1.0 - sig))).astype(jnp.bfloat16)
                a[here, pl.ds(hidden, hidden)] = (back * act).astype(jnp.bfloat16)
                ht[:, pl.ds(start, half)] = (act * up * columns[h]).T.astype(jnp.bfloat16)
            copy = remote(a.at[rows(s)], a_far.at[rows(s)], a_send.at[i], a_recv.at[i], partner)
            copy.start()
            a_copies.append(copy)

        def weight_copy(j, slot, part):
            target = (gg_out, gu_out)[j]
            return pltpu.make_async_copy(stage.at[slot, j], target.at[part], st_sem.at[slot, j])

        def down_copy(part):
            cols = pl.ds(pl.multiple_of(part * width, width), width)
            return pltpu.make_async_copy(wd.at[part], gd_out.at[:, cols], gd_sem.at[part])

        def weight_grads(first, stop):
            tile = 256

            @pl.loop(first, stop)
            def _(part):
                slot = lax.rem(part, 2)

                @pl.when(part >= 2)
                def _():
                    for j in (0, 1):
                        weight_copy(j, slot, part).wait()

                @pl.loop(0, width // tile)
                def _(n):
                    feats = pl.ds(pl.multiple_of(n * tile, tile), tile)
                    totals = [0.0, 0.0]
                    for g in range(groups):
                        here = pl.ds(g * tokens, tokens)
                        turned = xc[0, part, here, feats].T
                        for j in (0, 1):
                            totals[j] += dot_nn(turned, a[here, pl.ds(j * hidden, hidden)])
                    for j in (0, 1):
                        stage[slot, j, feats, :] = totals[j].astype(jnp.bfloat16)

                    wd[part, :, feats] = dot_nn(ht[...], xc[1, part, :, feats]).astype(jnp.bfloat16)

                for j in (0, 1):
                    weight_copy(j, slot, part).start()
                down_copy(part).start()

        chunks = 4
        span = tokens // chunks

        def part_rows(q):
            return pl.ds(pl.multiple_of(q * span, span), span)

        def partial(s, k, finish):
            layer = flip(z, k)
            value = dot_nt(a[rows(s), :], w[2 * layer + c]) + dot_nt(a_far[rows(s), :], wp[layer])
            finish[k] = value.astype(finish.dtype)

        def rs_copy(kind, k, q, device):
            source, target = ((sd, rd), (sx, rx), (sy, ry))[kind]
            return remote(
                source.at[k, part_rows(q)],
                target.at[k, part_rows(q)],
                rs_send.at[kind, k, q],
                rs_recv.at[kind, k, q],
                device,
            )

        def landed(kind, k, q):
            rs_copy(kind, k, q, partner).wait_recv()

        def wide(ref):
            return ref.astype(jnp.float32)

        def merge(kind, k, q):
            landed(0, k, q)
            here = part_rows(q)
            buffer = (None, sx, sy)[kind]
            buffer[k, here, :] = (wide(buffer[k, here, :]) + wide(rd[k, here, :])).astype(jnp.bfloat16)
            rs_copy(kind, k, q, (None, x_dev, y_dev)[kind]).start()

        def stage_a(q):
            rs_copy(0, 2, q, x_dev).start()
            rs_copy(0, 3, q, y_dev).start()
            rs_copy(1, 2, q, x_dev).start()
            rs_copy(2, 3, q, y_dev).start()
            rs_copy(0, 0, q, x_dev).start()
            rs_copy(0, 1, q, y_dev).start()

        def stage_b(q):
            merge(2, 2, q)
            merge(1, 3, q)
            rs_copy(1, 0, q, x_dev).start()
            rs_copy(2, 1, q, y_dev).start()

        def stage_c(q):
            merge(2, 0, q)
            merge(1, 1, q)

        def z_ship(k, q):
            to = flip(z, 1) if k == 1 else flip(z, 1 + 2 * mid)
            slot = {1: 0, 2: 3 + 2 * mid, 3: 2 + 2 * mid}[k]
            return remote(
                sz.at[k, part_rows(q)],
                rz.at[slot, part_rows(q)],
                z_send.at[k, q],
                z_recv.at[slot, q],
                (sp, 2 * to + c),
            )

        def z_landed(slot, q):
            remote(
                sz.at[0, part_rows(q)], rz.at[slot, part_rows(q)], z_send.at[0, q], z_recv.at[slot, q], partner
            ).wait_recv()

        def collect(k, q):
            landed(1, k, q)
            landed(2, k, q)
            here = part_rows(q)
            total = sums[k, here, :] + wide(rx[k, here, :]) + wide(ry[k, here, :])
            sums[k, here, :] = total
            if k:

                @pl.when(mid == 0)
                def _():
                    sz[k, here, :] = total.astype(jnp.bfloat16)
                    z_ship(k, q).start()

        def pass_along(k, q):
            here = part_rows(q)
            slot = {1: 5, 2: 2, 3: 3}[k]

            @pl.when(inner)
            def _():
                z_landed(slot, q)
                total = sums[k, here, :] + wide(rz[slot, here, :])
                sz[k, here, :] = total.astype(jnp.bfloat16)
                z_ship(k, q).start()

        def m_copy(q, part, slot, device):
            return remote(
                m.at[part, part_rows(q)],
                m.at[part, part_rows(q)],
                m_send.at[q, slot],
                m_recv.at[q, part],
                device,
            )

        def conclude(q):
            here = part_rows(q)
            z_landed(0, q)

            @pl.when(inner)
            def _():
                z_landed(4, q)

            mine = pl.ds(pl.multiple_of(sp * tokens + q * span, span), span)
            total = sums[0, here, :] + wide(xc[1, tp, mine, :])
            total += wide(rz[0, here, :]) + wide(rz[4, here, :])
            m[tp, here, :] = total.astype(jnp.bfloat16)
            for k in (3, 2, 1):
                m_copy(q, tp, k, z_dev(k)).start()
            m_copy(q, tp, 0, partner).start()

        def across(q, k):
            layer = flip(z, k)
            return layer != sp, remote(
                m.at[2 * layer + c, part_rows(q)],
                cols_in.at[sp, c, part_rows(q)],
                a2_send.at[q, k],
                a2_recv.at[q, sp],
                (layer, tp),
            )

        def beside(q, s, side):
            return remote(
                cols_in.at[s, side, part_rows(q)],
                cols_in.at[s, side, part_rows(q)],
                a2p_send.at[q, s],
                a2p_recv.at[q, s],
                partner,
            )

        def spread(q):
            for k in (0, 3, 2, 1):
                part = 2 * flip(z, k) + c
                if k:
                    m_copy(q, part, 0, partner).wait_recv()
                    m_copy(q, part, 3 + k, partner).start()
                needed, copy = across(q, k)

                @pl.when(needed)
                def _():
                    copy.start()

        def project(q):
            here = part_rows(q)
            for layer in range(layers):
                m_copy(q, 2 * layer + near, 0, partner).wait_recv()
            total = dot_nn(m[0, here, :], op[0])
            for part in range(1, parts):
                total += dot_nn(m[part, here, :], op[part])
            gm[here, :] = total

        def relay(q):
            for d in (1, 2, 3):
                s = lax.rem(sp + d, groups)
                remote(
                    m.at[tp, part_rows(q)], cols_in.at[s, c, part_rows(q)], a2_send.at[q, 0], a2_recv.at[q, s], partner
                ).wait_recv()
                beside(q, s, c).start()

        def partner_rows(i):
            a_copies[i].wait_recv()

        gate_rows(0, dn)
        gate_rows(1, xn)
        partner_rows(0)
        partial(dn, 2, sd)
        rs_copy(0, 2, 0, x_dev).start()
        partial(dn, 3, sd)
        rs_copy(0, 3, 0, y_dev).start()
        gate_rows(2, yn)
        partner_rows(1)
        partial(xn, 2, sx)
        rs_copy(1, 2, 0, x_dev).start()
        gate_rows(3, sp)
        partner_rows(2)
        partial(yn, 3, sy)
        rs_copy(2, 3, 0, y_dev).start()
        partial(dn, 0, sd)
        rs_copy(0, 0, 0, x_dev).start()
        partial(dn, 1, sd)
        rs_copy(0, 1, 0, y_dev).start()
        stage_a(1)
        partner_rows(3)
        partial(yn, 2, sy)
        partial(xn, 3, sx)
        partial(xn, 0, sx)
        partial(yn, 1, sy)
        mixed_copies = [
            remote(mixed.at[sp], mixed.at[sp], mx_send.at[i], mx_recv.at[sp], device)
            for i, device in enumerate((x_dev, y_dev, d_dev))
        ]

        def during(q, first, last, work):
            @pl.when((q >= first) & (q <= last))
            def _():
                work(q - first)

        def round_trip(q, carry):
            @pl.when(q == 0)
            def _():
                stage_b(0)
                partial(yn, 0, sy)
                partial(xn, 1, sx)
                stage_c(0)
                stage_a(2)
                for k in (3, 2, 1, 0):
                    partial(sp, k, sums)

            def ends(i):
                collect(1, i)
                collect(0, i)

            during(q, 1, chunks, ends)
            during(q, 2, chunks + 1, conclude)
            during(q, 3, chunks + 2, spread)
            during(q, 1, chunks - 1, lambda i: stage_b(i + 1))

            def handed(i):
                pass_along(2, i)
                pass_along(3, i)

            during(q, 1, chunks, handed)
            during(q, 0, chunks - 1, lambda i: weight_grads(2 * i, 2 * i + 1))
            during(q, 1, chunks - 1, lambda i: stage_c(i + 1))

            @pl.when(q == 1)
            def _():
                stage_a(3)


            @pl.when(q == chunks - 1)
            def _():
                for copy in mixed_copies:
                    copy.start()

            def middle_collect(i):
                collect(3, i)
                collect(2, i)

            during(q, 0, chunks - 1, middle_collect)
            during(q, 1, chunks, lambda i: pass_along(1, i))
            during(q, 0, chunks - 1, lambda i: weight_grads(2 * i + 1, 2 * i + 2))
            during(q, 4, chunks + 3, project)
            during(q, 4, chunks + 3, relay)
            return carry

        op_load.wait()
        lax.fori_loop(0, chunks + 4, round_trip, 0)
        gc[middle, :] = gm[...] * gates[0].astype(jnp.float32)
        gc_edges = edges(gc, 1)
        for copy in gc_edges:
            copy.start()
        outs_v[0] = (gm[...] * conv[...]).astype(jnp.bfloat16)
        finals = [pltpu.make_async_copy(outs_v.at[0], gog_out, out_sem.at[3])]
        finals[0].start()
        for s in (xn, yn, dn):
            remote(mixed.at[s], mixed.at[s], mx_send.at[0], mx_recv.at[s], partner).wait_recv()

        @pl.loop(0, chunks)
        def _(q):
            for d in (1, 2, 3):
                beside(q, lax.rem(sp + d, groups), near).wait_recv()


        tile = width // 2

        @pl.loop(0, 2)
        def _(side):
            @pl.loop(0, 2)
            def _(n):
                feats = pl.ds(pl.multiple_of(n * tile, tile), tile)
                total = dot_nn(m[2 * sp + side, :, feats].T, mixed[sp])
                for d in (1, 2, 3):
                    s = lax.rem(sp + d, groups)
                    total += dot_nn(cols_in[s, side, :, feats].T, mixed[s])
                acc[pl.ds(pl.multiple_of(side * width + n * tile, tile), tile), :] = total

        copy = pltpu.make_async_copy(acc, gop_out, out_sem.at[4])
        copy.start()
        finals.append(copy)
        close_edges(gc, gc_edges)
        grad = (
            gc[pl.ds(pad + 1, tokens), :] * taps[0:1, :]
            + gc[middle, :] * taps[1:2, :]
            + gc[pl.ds(pad - 1, tokens), :] * taps[2:3, :]
        )
        outs_v[1] = (grad * gates[2].astype(jnp.float32)).astype(jnp.bfloat16)
        outs_v[2] = (grad * gates[1].astype(jnp.float32)).astype(jnp.bfloat16)
        for j, target in ((1, gig_out), (2, gva_out)):
            copy = pltpu.make_async_copy(outs_v.at[j], target, out_sem.at[5 + j])
            copy.start()
            finals.append(copy)
        for copy in a_copies + mixed_copies + ci_edges + gc_edges:
            copy.wait_send()

        @pl.loop(0, chunks)
        def _(q):
            for kind, ks in ((0, range(4)), (1, range(4)), (2, range(4))):
                for k in ks:
                    rs_copy(kind, k, q, partner).wait_send()
            for slot in range(7):
                m_copy(q, tp, slot, partner).wait_send()
            for k in (1, 2, 3):
                z_ship(k, q).wait_send()
            for k in range(4):
                needed, copy = across(q, k)

                @pl.when(needed)
                def _():
                    copy.wait_send()

            for d in (1, 2, 3):
                beside(q, lax.rem(sp + d, groups), c).wait_send()

        for t in (0, 1):

            def sent(slot):
                pass_on(t, sp, tp, slot, partner).wait_send()

            pl.loop(0, 13)(sent)
            pl.loop(15, 27)(sent)
            if t:
                sent(31)
                sent(35)
            else:
                pl.loop(31, 35)(sent)

            @pl.when(inner)
            def _():
                sent(13)
                pl.loop(28, 31)(sent)
                if t:
                    pl.loop(36, 40)(sent)

        for slot in (0, 1):
            for j in (0, 1):
                weight_copy(j, slot, slot).wait()
        for part in range(parts):
            down_copy(part).wait()
        for copy in finals:
            copy.wait()

    block_shape = (layers, tokens, width)
    shapes = [
        jax.ShapeDtypeStruct((parts, width, hidden), jnp.bfloat16),
        jax.ShapeDtypeStruct((parts, width, hidden), jnp.bfloat16),
        jax.ShapeDtypeStruct((hidden, parts * width), jnp.bfloat16),
    ]
    shapes += [jax.ShapeDtypeStruct((tokens, width), jnp.bfloat16)] * 3
    shapes.append(jax.ShapeDtypeStruct((2 * width, width), jnp.float32))
    half = jnp.bfloat16
    return pl.pallas_call(
        kernel,
        out_shape=shapes,
        in_specs=[pl.BlockSpec(memory_space=pl.ANY)] * 9
        + [pl.BlockSpec(memory_space=pltpu.VMEM), pl.BlockSpec(memory_space=pl.ANY)],
        out_specs=[pl.BlockSpec(memory_space=pl.ANY)] * 7,
        scratch_shapes=[
            pltpu.VMEM((2, parts, rows_all, width), half),
            pltpu.VMEM((parts, width, 2 * hidden), half),
            pltpu.VMEM((parts, hidden, width), half),
            pltpu.VMEM((layers, width, 2 * hidden), half),
            pltpu.VMEM((rows_all, 2 * hidden), jnp.float32),
            pltpu.VMEM((rows_all, hidden), jnp.float32),
            pltpu.VMEM((rows_all, 2 * hidden), half),
            pltpu.VMEM((rows_all, 2 * hidden), half),
            pltpu.VMEM((hidden, rows_all), half),
            pltpu.VMEM((2, 2, width, hidden), half),
            pltpu.VMEM((groups, 8, tokens), jnp.float32),
            pltpu.VMEM(block_shape, jnp.float32),
        ]
        + [pltpu.VMEM(block_shape, half)] * 7
        + [
            pltpu.VMEM((6, tokens, width), half),
            pltpu.VMEM((parts, width, width), half),
            pltpu.VMEM((parts, tokens, width), half),
            pltpu.VMEM((groups, 2, tokens, width), half),
            pltpu.VMEM((groups, tokens, width), half),
            pltpu.VMEM((tokens + 16, width), jnp.float32),
            pltpu.VMEM((tokens + 16, width), jnp.float32),
            pltpu.VMEM((tokens, width), jnp.float32),
            pltpu.VMEM((tokens, width), jnp.float32),
            pltpu.VMEM((3, tokens, width), half),
            pltpu.VMEM((3, tokens, width), half),
            pltpu.SemaphoreType.DMA((9 + parts,)),
            pltpu.SemaphoreType.DMA((2, 40)),
            pltpu.SemaphoreType.DMA((2, groups, parts)),
            pltpu.SemaphoreType.DMA((3,)),
            pltpu.SemaphoreType.DMA((3,)),
            pltpu.SemaphoreType.DMA((layers,)),
            pltpu.SemaphoreType.DMA((layers,)),
            pltpu.SemaphoreType.DMA((groups,)),
            pltpu.SemaphoreType.DMA((groups,)),
            pltpu.SemaphoreType.DMA((3, layers, 4)),
            pltpu.SemaphoreType.DMA((3, layers, 4)),
            pltpu.SemaphoreType.DMA((layers, 4)),
            pltpu.SemaphoreType.DMA((6, 4)),
            pltpu.SemaphoreType.DMA((8,)),
            pltpu.SemaphoreType.DMA((2, 2)),
            pltpu.SemaphoreType.DMA((parts,)),
            pltpu.SemaphoreType.DMA((2, 2)),
            pltpu.SemaphoreType.DMA((2, 2)),
            pltpu.SemaphoreType.DMA((3,)),
            pltpu.SemaphoreType.DMA((groups,)),
            pltpu.SemaphoreType.DMA((4, 7)),
            pltpu.SemaphoreType.DMA((4, parts)),
            pltpu.SemaphoreType.DMA((4, layers)),
            pltpu.SemaphoreType.DMA((4, groups)),
            pltpu.SemaphoreType.DMA((4, groups)),
            pltpu.SemaphoreType.DMA((4, groups)),
        ],
        compiler_params=pltpu.CompilerParams(
            collective_id=10, has_side_effects=True, vmem_limit_bytes=62 * 1024 * 1024
        ),
    )


def finish(grads, rest):
    pieces = 4
    count, total = (len(grads), len(grads) + len(rest))

    def kernel(*refs):
        sources, targets = (refs[:total], refs[total : 2 * total])
        narrow, broad = (refs[2 * total : 2 * total + count], refs[2 * total + count : 2 * total + 2 * count])
        through = refs[2 * total + 2 * count : 3 * total + count]
        in_sem, out_sem = refs[-2:]

        def piece(ref, i):
            size = ref.shape[0] // pieces
            return ref.at[pl.ds(i * size, size)]

        fetches = {}
        for i in range(pieces):
            for j in range(count):
                fetches[i, j] = pltpu.make_async_copy(
                    piece(sources[j], i), piece(narrow[j], i), in_sem.at[j, i]
                )
                fetches[i, j].start()
        for j in range(count, total):
            fetches[0, j] = pltpu.make_async_copy(sources[j], through[j - count], in_sem.at[j, 0])
            fetches[0, j].start()
        stores = []

        def store(source, target, j, i):
            copy = pltpu.make_async_copy(source, target, out_sem.at[j, i])
            copy.start()
            stores.append(copy)

        for i in range(pieces):
            for j in range(count):
                fetches[i, j].wait()
                size = narrow[j].shape[0] // pieces
                steps = 4
                rows = size // steps

                @pl.loop(0, steps)
                def _(n):
                    here = pl.ds(pl.multiple_of(i * size + n * rows, rows), rows)
                    broad[j][here, :] = narrow[j][here, :].astype(jnp.float32)

                store(piece(broad[j], i), piece(targets[j], i), j, i)
        for j in range(count, total):
            fetches[0, j].wait()
            store(through[j - count], targets[j], j, 0)
        for copy in stores:
            copy.wait()

    shapes = [jax.ShapeDtypeStruct(g.shape, jnp.float32) for g in grads]
    shapes += [jax.ShapeDtypeStruct(r.shape, r.dtype) for r in rest]
    return pl.pallas_call(
        kernel,
        out_shape=shapes,
        in_specs=[pl.BlockSpec(memory_space=pl.ANY)] * total,
        out_specs=[pl.BlockSpec(memory_space=pl.ANY)] * total,
        scratch_shapes=[pltpu.VMEM(g.shape, g.dtype) for g in grads]
        + [pltpu.VMEM(g.shape, jnp.float32) for g in grads]
        + [pltpu.VMEM(r.shape, r.dtype) for r in rest]
        + [pltpu.SemaphoreType.DMA((total, pieces))] * 2,
        compiler_params=pltpu.CompilerParams(vmem_limit_bytes=62 * 1024 * 1024),
    )(*grads, *rest)


def near_body(
    moe_input,
    out_gate,
    in_gate,
    values,
    conv_taps,
    out_proj,
    route_ids,
    route_gates,
    expert_gate,
    expert_up,
    expert_down,
    cotangent,
):
    token_count, part_width = moe_input.shape
    group_count = lax.axis_size("sp")
    hidden = expert_gate.shape[2]
    part_count = lax.axis_size("tp")
    chosen = route_ids[None, :, :] == jnp.arange(group_count, dtype=jnp.int32)[:, None, None]
    weights = jnp.sum(jnp.where(chosen, route_gates[None, :, :], 0.0), axis=2)
    route = jnp.broadcast_to(weights[:, None, :], (group_count, 8, token_count))
    (
        grad_expert_gate,
        grad_expert_up,
        grad_expert_down,
        grad_out_gate,
        grad_in_gate,
        grad_values,
        grad_out_proj,
    ) = experts_kernel(token_count, part_width, hidden)(
        moe_input,
        cotangent,
        route,
        expert_gate.reshape(part_count, part_width, hidden),
        expert_up.reshape(part_count, part_width, hidden),
        expert_down[0],
        out_gate,
        in_gate,
        values,
        conv_taps,
        out_proj.reshape(part_count, part_width, part_width),
    )

    (
        grad_expert_gate,
        grad_expert_up,
        grad_expert_down,
        grad_out_gate,
        grad_in_gate,
        grad_values,
        grad_out_proj,
    ) = finish(
        (
            grad_expert_gate.reshape(-1, hidden),
            grad_expert_up.reshape(-1, hidden),
            grad_expert_down,
        ),
        (grad_out_gate, grad_in_gate, grad_values, grad_out_proj),
    )
    grad_expert_gate = grad_expert_gate[None]
    grad_expert_up = grad_expert_up[None]
    grad_expert_down = grad_expert_down[None]
    return (
        grad_out_gate,
        grad_in_gate,
        grad_values,
        grad_out_proj,
        grad_expert_gate,
        grad_expert_up,
        grad_expert_down,
    )


def step(*arrays):
    moe_input, expert_gate, out_proj = (arrays[0], arrays[8], arrays[5])
    tokens, width = moe_input.shape
    near = (
        lax.axis_size("sp") == 4
        and lax.axis_size("tp") == 8
        and expert_gate.shape[0] == 1
        and tokens % 256 == 0
        and width == 2 * expert_gate.shape[2] == 2 * tokens
        and out_proj.shape[0] == 8 * width
    )
    return (near_body if near else body)(*arrays)


def solution(mesh):
    return jax.shard_map(
        step,
        mesh=mesh,
        in_specs=(
            P("sp", "tp"),
            P("sp", "tp"),
            P("sp", "tp"),
            P("sp", "tp"),
            P(None, "tp"),
            P(None, "tp"),
            P("sp", None),
            P("sp", None),
            P("sp", None, "tp"),
            P("sp", None, "tp"),
            P("sp", "tp", None),
            P("sp", "tp"),
        ),
        out_specs=(
            P("sp", "tp"),
            P("sp", "tp"),
            P("sp", "tp"),
            P("sp", "tp"),
            P("sp", None, "tp"),
            P("sp", None, "tp"),
            P("sp", "tp", None),
        ),
        check_vma=False,
    )
```

```python
import jax
import jax.numpy as jnp
from jax import lax
from jax.experimental import pallas as pl
from jax.experimental.pallas import tpu as pltpu
from jax.sharding import PartitionSpec as P

MESH = pl.DeviceIdType.MESH


def peers_of(group):
    sp, tp = (lax.axis_index("sp"), lax.axis_index("tp"))
    if group == "core":
        me, size = (lax.rem(tp, 2), 2)
    elif group == "z":
        me, size = (lax.div(tp, 2), lax.axis_size("tp") // 2)
    else:
        me, size = (sp, lax.axis_size("sp"))
    others = []
    for k in range(1, size):
        place = lax.rem(me + k, size)
        if group == "core":
            others.append((place, (sp, tp - me + place)))
        elif group == "z":
            others.append((place, (sp, place * 2 + lax.rem(tp, 2))))
        else:
            others.append((place, (place, tp)))
    return me, others


def group_size(group):
    if group == "core":
        return 2
    return lax.axis_size("tp") // 2 if group == "z" else lax.axis_size("sp")


def block(ref, place, width):
    return ref.at[:, pl.ds(pl.multiple_of(place * width, width), width)]


def exchange(collective_id, *ops):
    arrays = [op[2] for op in ops]
    shapes = []
    counts = []
    for kind, group, array, *rest in ops:
        size = group_size(group)
        if kind == "cores":
            shape, count = ((array.shape[0], array.shape[1] // 2), array.shape[1] // rest[0] // 2)
        elif kind == "columns":
            shape = (size - 1, array.shape[0], array.shape[1] // size)
            count = size - 1
        elif kind == "rows":
            shape, count = ((size - 1,) + array.shape[1:], size - 1)
        elif kind == "gather":
            shape, count = ((array.shape[0], array.shape[1] * size), size - 1)
        elif kind == "send":
            shape, count = (array.shape, size - 1)
        elif kind == "stack":
            shape, count = ((size,) + array.shape, size - 1)
        else:
            shape, count = (array.shape, 1)
        shapes.append(jax.ShapeDtypeStruct(shape, array.dtype))
        counts.append(count)
    total = sum(counts)

    def kernel(*refs):
        n = len(ops)
        sources, targets = (refs[:n], refs[n : 2 * n])
        send_sem, recv_sem, own_sem = refs[2 * n :]
        barrier = pltpu.get_barrier_semaphore()
        greeted = 0
        for group in sorted({op[1] for op in ops}):
            for _, device in peers_of(group)[1]:
                pl.semaphore_signal(barrier, inc=1, device_id=device, device_id_type=MESH)
                greeted += 1
        pl.semaphore_wait(barrier, greeted)
        copies = []
        local = []
        for i, (kind, group, array, *rest) in enumerate(ops):
            me, others = peers_of(group)
            source, target = (sources[i], targets[i])
            moves = []
            if kind == "cores":
                width = rest[0]
                place, device = others[0]
                for b in range(counts[i]):
                    moves.append(
                        (
                            block(source, 2 * b + place, width),
                            target.at[:, pl.ds(b * width, width)],
                            device,
                        )
                    )
            for k, (place, device) in enumerate(others):
                if kind == "columns":
                    moves.append((block(source, place, shapes[i].shape[2]), target.at[k], device))
                elif kind == "rows":
                    moves.append((source.at[place], target.at[k], device))
                elif kind == "gather":
                    moves.append((source, block(target, me, array.shape[1]), device))
                elif kind == "send":
                    moves.append((source.at[place], target.at[me], device))
                elif kind == "stack":
                    moves.append((source, target.at[me], device))
                elif kind == "swap":
                    moves.append((source, target, device))
            for a, b, device in moves:
                j = len(copies)
                copy = pltpu.make_async_remote_copy(
                    src_ref=a,
                    dst_ref=b,
                    send_sem=send_sem.at[j],
                    recv_sem=recv_sem.at[j],
                    device_id=device,
                    device_id_type=MESH,
                )
                copy.start()
                copies.append(copy)
            if kind == "gather":
                local.append((source, block(target, me, array.shape[1]), i))
            elif kind == "send":
                local.append((source.at[me], target.at[me], i))
            elif kind == "stack":
                local.append((source, target.at[me], i))
        own = [pltpu.make_async_copy(a, b, own_sem.at[i]) for a, b, i in local]
        for copy in own:
            copy.start()
        for copy in own + copies:
            copy.wait()

    return pl.pallas_call(
        kernel,
        out_shape=shapes,
        in_specs=[pl.BlockSpec(memory_space=pl.ANY)] * len(ops),
        out_specs=[pl.BlockSpec(memory_space=pl.ANY)] * len(ops),
        scratch_shapes=[
            pltpu.SemaphoreType.DMA((total,)),
            pltpu.SemaphoreType.DMA((total,)),
            pltpu.SemaphoreType.DMA((len(ops),)),
        ],
        compiler_params=pltpu.CompilerParams(collective_id=collective_id, has_side_effects=True),
    )(*arrays)


def halves(array, width):
    core = lax.rem(lax.axis_index("tp"), 2)
    blocks = [
        lax.dynamic_slice_in_dim(array, (start + core) * width, width, axis=1)
        for start in range(0, array.shape[1] // width, 2)
    ]
    return jnp.concatenate(blocks, axis=1)


def interleave(own, other, width):
    core = lax.rem(lax.axis_index("tp"), 2)
    first, second = (jnp.where(core == 0, own, other), jnp.where(core == 0, other, own))
    blocks = []
    for start in range(0, own.shape[1], width):
        blocks.append(first[:, start : start + width])
        blocks.append(second[:, start : start + width])
    return jnp.concatenate(blocks, axis=1)


def padded(array, sides, width):
    for axis, dim in sides:
        size, length = (lax.axis_size(axis), array.shape[dim])
        up = [(i, (i + 1) % size) for i in range(size - 1)]
        down = [(j, i) for i, j in up]
        last = lax.slice_in_dim(array, length - width, length, axis=dim)
        initial = lax.slice_in_dim(array, 0, width, axis=dim)
        before = lax.ppermute(last, axis, up)
        after = lax.ppermute(initial, axis, down)
        array = jnp.concatenate([before, array, after], axis=dim)
    return array


def body(
    moe_input,
    out_gate,
    in_gate,
    values,
    conv_taps,
    out_proj,
    route_ids,
    route_gates,
    expert_gate,
    expert_up,
    expert_down,
    cotangent,
):
    token_count = moe_input.shape[0]
    part_width = moe_input.shape[1]
    pick_count = route_ids.shape[1]
    group_count = lax.axis_size("sp")
    local_count = expert_gate.shape[0]
    expert_count = group_count * local_count
    capacity = 3 * token_count // expert_count
    contract_rows = (((0,), (0,)), ((), ()))
    flat_ids = route_ids.reshape(-1)
    one_hot = (flat_ids[:, None] == jnp.arange(expert_count, dtype=jnp.int32)[None, :]).astype(
        jnp.int32
    )
    earlier = jnp.cumsum(one_hot, axis=0) - one_hot
    position = jnp.sum(earlier * one_hot, axis=1)
    slot_index = flat_ids * capacity + position
    block_rows = local_count * capacity
    slots = jnp.arange(expert_count * capacity, dtype=jnp.int32)
    hits = slots[:, None, None] == slot_index.reshape(token_count, pick_count)[None, :, :]
    take = jnp.any(hits, axis=2).astype(jnp.bfloat16)
    slot_weight = jnp.sum(jnp.where(hits, route_gates[None, :, :], 0.0), axis=(1, 2))
    conv_in = in_gate.astype(jnp.float32) * values.astype(jnp.float32)
    rimmed = padded(conv_in, (("sp", 0),), 1)
    conv_out = rimmed[:-2] * conv_taps[0] + rimmed[1:-1] * conv_taps[1] + rimmed[2:] * conv_taps[2]
    mixed = (out_gate.astype(jnp.float32) * conv_out).astype(jnp.bfloat16)
    rows_z, mixed_all = exchange(4, ("gather", "z", moe_input), ("stack", "sp", mixed))
    half = rows_z.shape[1]
    send_rows = jnp.dot(take, rows_z, preferred_element_type=jnp.float32).astype(jnp.bfloat16)
    cot_z, recv_rows = exchange(
        5,
        ("gather", "z", cotangent),
        ("send", "sp", send_rows.reshape(group_count, block_rows, half)),
    )
    send_cot = (
        slot_weight[:, None] * jnp.dot(take, cot_z, preferred_element_type=jnp.float32)
    ).astype(jnp.bfloat16)
    recv_rows = recv_rows.reshape(group_count * block_rows, half)
    recv_cot, swap_rows = exchange(
        6,
        ("send", "sp", send_cot.reshape(group_count, block_rows, half)),
        ("swap", "core", recv_rows),
    )
    recv_cot = recv_cot.reshape(group_count * block_rows, half)
    (swap_cot,) = exchange(7, ("swap", "core", recv_cot))

    def by_expert(own, other):
        full = interleave(own, other, part_width)
        full = full.reshape(group_count, local_count, capacity, 2 * half)
        return jnp.swapaxes(full, 0, 1).reshape(local_count, group_count * capacity, 2 * half)

    full_rows = by_expert(recv_rows, swap_rows)
    full_cot = by_expert(recv_cot, swap_cot)
    pre_gate = jnp.einsum(
        "prd,pdf->prf", full_rows, expert_gate, preferred_element_type=jnp.float32
    )
    pre_up = jnp.einsum("prd,pdf->prf", full_rows, expert_up, preferred_element_type=jnp.float32)
    gate_sig = jax.nn.sigmoid(pre_gate)
    activated = pre_gate * gate_sig
    hidden_act = (activated * pre_up).astype(jnp.bfloat16)
    grad_expert_down = jnp.einsum(
        "prf,prd->pfd", hidden_act, full_cot, preferred_element_type=jnp.float32
    )
    grad_hidden = jnp.einsum(
        "prd,pfd->prf", full_cot, expert_down, preferred_element_type=jnp.float32
    )
    grad_pre_gate = (grad_hidden * pre_up * gate_sig * (1.0 + pre_gate * (1.0 - gate_sig))).astype(
        jnp.bfloat16
    )
    grad_pre_up = (grad_hidden * activated).astype(jnp.bfloat16)
    grad_expert_gate = jnp.einsum(
        "prd,prf->pdf", full_rows, grad_pre_gate, preferred_element_type=jnp.float32
    )
    grad_expert_up = jnp.einsum(
        "prd,prf->pdf", full_rows, grad_pre_up, preferred_element_type=jnp.float32
    )
    partial_grad = jnp.einsum(
        "prf,pdf->prd", grad_pre_gate, expert_gate, preferred_element_type=jnp.float32
    ) + jnp.einsum("prf,pdf->prd", grad_pre_up, expert_up, preferred_element_type=jnp.float32)
    me = lax.axis_index("sp")
    partial_rows = partial_grad.astype(jnp.bfloat16).reshape(local_count * group_count * capacity, -1)
    (other_core,) = exchange(1, ("cores", "core", partial_rows, part_width))
    chip_rows = (
        halves(partial_rows, part_width).astype(jnp.float32) + other_core.astype(jnp.float32)
    ).astype(jnp.bfloat16)
    chip_rows = jnp.swapaxes(
        chip_rows.reshape(local_count, group_count, capacity, half), 0, 1
    ).reshape(group_count, block_rows, half)
    (returned,) = exchange(2, ("rows", "sp", chip_rows))
    back = lax.rem(me - jnp.arange(group_count) + group_count, group_count)
    local_slots = jnp.arange(block_rows, dtype=jnp.int32)
    picks = jnp.sum(
        (slot_index.reshape(token_count, pick_count)[None, :, :, None])
        == (back[:, None] * block_rows + local_slots)[:, None, None, :],
        axis=2,
    ).astype(jnp.bfloat16)
    token_part = jnp.dot(
        picks[0],
        lax.dynamic_index_in_dim(chip_rows, me, 0, keepdims=False),
        preferred_element_type=jnp.float32,
    ) + jnp.einsum("kts,ksd->td", picks[1:], returned, preferred_element_type=jnp.float32)
    token_part = token_part.astype(jnp.bfloat16)
    (parts,) = exchange(3, ("columns", "z", token_part))
    own_part = lax.dynamic_slice_in_dim(
        token_part, lax.div(lax.axis_index("tp"), 2) * part_width, part_width, axis=1
    )
    moe_grad = own_part.astype(jnp.float32) + jnp.sum(parts.astype(jnp.float32), axis=0)
    mixer_cot = (cotangent.astype(jnp.float32) + moe_grad).astype(jnp.bfloat16)
    (mixer_z,) = exchange(8, ("gather", "z", mixer_cot))
    (mixer_other,) = exchange(9, ("swap", "core", mixer_z))
    full_mixer_cot = interleave(mixer_z, mixer_other, part_width)
    grad_mixed = jnp.dot(full_mixer_cot, out_proj, preferred_element_type=jnp.float32)
    grad_out_gate = (grad_mixed * conv_out).astype(jnp.bfloat16)
    grad_conv_out = grad_mixed * out_gate.astype(jnp.float32)
    rim_grad = padded(grad_conv_out, (("sp", 0),), 1)
    grad_conv_in = (
        rim_grad[2:] * conv_taps[0] + rim_grad[1:-1] * conv_taps[1] + rim_grad[:-2] * conv_taps[2]
    )
    grad_in_gate = (grad_conv_in * values.astype(jnp.float32)).astype(jnp.bfloat16)
    grad_values = (grad_conv_in * in_gate.astype(jnp.float32)).astype(jnp.bfloat16)
    columns = lax.all_to_all(full_mixer_cot, "sp", split_axis=1, concat_axis=0, tiled=True)
    grad_out_proj = lax.dot_general(
        columns,
        mixed_all.reshape(group_count * token_count, part_width),
        contract_rows,
        preferred_element_type=jnp.float32,
    )
    return (
        grad_out_gate,
        grad_in_gate,
        grad_values,
        grad_out_proj,
        grad_expert_gate,
        grad_expert_up,
        grad_expert_down,
    )


def flip(index, bits):
    high, low = (lax.div(index, 2), lax.rem(index, 2))
    bit_high, bit_low = (lax.div(bits, 2), lax.rem(bits, 2)) if not isinstance(bits, int) else (bits // 2, bits % 2)
    high = high + bit_high - 2 * high * bit_high
    low = low + bit_low - 2 * low * bit_low
    return 2 * high + low


def place():
    sp, tp = (lax.axis_index("sp"), lax.axis_index("tp"))
    return sp, lax.div(tp, 2), lax.rem(tp, 2)


def greet(devices):
    barrier = pltpu.get_barrier_semaphore()
    for device in devices:
        pl.semaphore_signal(barrier, inc=1, device_id=device, device_id_type=MESH)
    pl.semaphore_wait(barrier, len(devices))


def remote(source, target, send_sem, recv_sem, device):
    return pltpu.make_async_remote_copy(
        src_ref=source,
        dst_ref=target,
        send_sem=send_sem,
        recv_sem=recv_sem,
        device_id=device,
        device_id_type=MESH,
    )


def dot_nt(a, b):
    return lax.dot_general(a, b, (((1,), (1,)), ((), ())), preferred_element_type=jnp.float32)


def dot_nn(a, b):
    return jnp.dot(a, b, preferred_element_type=jnp.float32)


def dot_tn(a, b):
    return lax.dot_general(a, b, (((0,), (0,)), ((), ())), preferred_element_type=jnp.float32)


def experts_kernel(tokens, width, hidden):
    groups, layers = (4, 4)
    parts = 2 * layers
    rows_all = groups * tokens

    def kernel(
        x_hbm, c_hbm, route, wg_hbm, wu_hbm, wd_hbm, og_hbm, ig_hbm, va_hbm, taps, op_hbm,
        gg_out, gu_out, gd_out, gog_out, gig_out, gva_out, gop_out,
        xc, w, wd, wp, acc, acc_down, a, a_far, ht, stage, wrow, sums,
        sd, sx, sy, sz, rd, rx, ry, rz,
        op, m, cols_in, mixed, ci, gc, conv, gm, gates, outs_v,
        load, xc_send, xc_recv, wr_send, wr_recv, wp_send, wp_recv, a_send, a_recv,
        rs_send, rs_recv, z_send, z_recv, out_sem, st_sem, gd_sem,
        edge_send, edge_recv, mx_send, mx_recv, m_send, m_recv, a2_send, a2_recv, a2p_send, a2p_recv,
    ):
        sp, z, c = place()
        tp = 2 * z + c
        xn, yn, dn = (flip(sp, 1), flip(sp, 2), flip(sp, 3))
        near = 1 - c
        partner = (sp, 2 * z + near)
        x_dev, y_dev, d_dev = ((xn, tp), (yn, tp), (dn, tp))

        mid = lax.rem(lax.div(z, 2) + lax.rem(z, 2), 2)
        inner = mid == 1

        def z_dev(k):
            return (sp, 2 * flip(z, k) + c)

        def rows(s):
            return pl.ds(pl.multiple_of(s * tokens, tokens), tokens)

        def blk(t, s, part):
            return xc.at[t, part, rows(s)]

        loads = [
            pltpu.make_async_copy(x_hbm, blk(0, sp, tp), load.at[0]),
            pltpu.make_async_copy(c_hbm, blk(1, sp, tp), load.at[1]),
            pltpu.make_async_copy(wg_hbm, w.at[:, :, pl.ds(0, hidden)], load.at[2]),
            pltpu.make_async_copy(wu_hbm, w.at[:, :, pl.ds(hidden, hidden)], load.at[3]),
            pltpu.make_async_copy(route.at[sp], wrow.at[sp], load.at[4]),
        ]
        for part in range(parts):
            loads.append(
                pltpu.make_async_copy(
                    wd_hbm.at[:, pl.ds(part * width, width)], wd.at[part], load.at[5 + part]
                )
            )
        conv_loads = [
            pltpu.make_async_copy(source, gates.at[j], load.at[5 + parts + j])
            for j, source in enumerate((og_hbm, ig_hbm, va_hbm))
        ]
        op_load = pltpu.make_async_copy(op_hbm, op, load.at[8 + parts])
        for copy in loads[:2] + conv_loads + loads[2:] + [op_load]:
            copy.start()
        pad = 8
        middle = pl.ds(pad, tokens)

        def edges(buffer, phase):
            before, after = (lax.rem(sp + groups - 1, groups), lax.rem(sp + 1, groups))
            top, low = (pl.ds(0, pad), pl.ds(pad + tokens, pad))
            first, final = (pl.ds(pad, pad), pl.ds(tokens, pad))
            return [
                remote(
                    buffer.at[final], buffer.at[top], edge_send.at[phase, 0], edge_recv.at[phase, 0], (after, tp)
                ),
                remote(
                    buffer.at[first], buffer.at[low], edge_send.at[phase, 1], edge_recv.at[phase, 1], (before, tp)
                ),
            ]

        def close_edges(buffer, copies):
            for copy in copies:
                copy.wait_recv()

            @pl.when(sp == 0)
            def _():
                buffer[pl.ds(0, pad), :] = jnp.zeros((pad, width), jnp.float32)

            @pl.when(sp == groups - 1)
            def _():
                buffer[pl.ds(pad + tokens, pad), :] = jnp.zeros((pad, width), jnp.float32)

        ci_edges = edges(ci, 0)
        greet([partner, z_dev(1), z_dev(2), z_dev(3), x_dev, y_dev, d_dev])
        loads[0].wait()
        loads[1].wait()

        def pass_on(t, s, part, slot, device):
            return remote(
                blk(t, s, part), blk(t, s, part), xc_send.at[t, slot], xc_recv.at[t, s, part], device
            )

        def pass_half(s, part, h, slot, device):
            here = pl.ds(pl.multiple_of(s * tokens + h * (tokens // 2), tokens // 2), tokens // 2)
            block = xc.at[1, part, here]
            return remote(block, block, xc_send.at[1, slot], xc_recv.at[1, s, part], device)

        def arrive(t, s, part):
            pass_on(t, s, part, 0, partner).wait_recv()

        for t in (0, 1):
            pass_on(t, sp, tp, 12, z_dev(1)).start()

            @pl.when(inner)
            def _():
                pass_on(t, sp, tp, 13, z_dev(3)).start()

            pass_on(t, sp, tp, 4, x_dev).start()
            pass_on(t, sp, tp, 8, y_dev).start()
            pass_on(t, sp, tp, 0, partner).start()
        for copy in conv_loads:
            copy.wait()
        ci[middle, :] = gates[1].astype(jnp.float32) * gates[2].astype(jnp.float32)
        for copy in ci_edges:
            copy.start()
        route_copies = []
        for i, (s, device) in enumerate(((xn, x_dev), (yn, y_dev), (dn, d_dev))):
            copy = remote(route.at[s], wrow.at[sp], wr_send.at[i], wr_recv.at[i], device)
            copy.start()
            route_copies.append(copy)
        for copy in loads[2:]:
            copy.wait()
        weight_copies = []
        for part in range(layers):
            copy = remote(w.at[2 * part + near], wp.at[part], wp_send.at[part], wp_recv.at[part], partner)
            copy.start()
            weight_copies.append(copy)
        acc[...] = jnp.zeros_like(acc)
        acc_down[...] = jnp.zeros_like(acc_down)

        @pl.when(mid == 0)
        def _():
            rz[...] = jnp.zeros_like(rz)

        def multiply(t, layer):
            @pl.when(t == 0)
            def _():
                @pl.loop(0, groups)
                def _(s):
                    here = rows(s)
                    acc[here, :] += dot_nn(xc[0, 2 * layer, here, :], w[2 * layer]) + dot_nn(
                        xc[0, 2 * layer + 1, here, :], w[2 * layer + 1]
                    )

            @pl.when(t == 1)
            def _():
                @pl.loop(0, groups)
                def _(s):
                    here = rows(s)
                    acc_down[here, :] += dot_nt(xc[1, 2 * layer, here, :], wd[2 * layer]) + dot_nt(
                        xc[1, 2 * layer + 1, here, :], wd[2 * layer + 1]
                    )

        def turn(i):
            return flip(z, i + mid * lax.div(i, 2) * (5 - 2 * i))

        def step(i, carry):
            r, t = (lax.div(i, 2), lax.rem(i, 2))

            def onward(s, part, m, slot):
                @pl.when(inner & (m == 1))
                def _():
                    pass_on(t, s, part, slot, z_dev(3)).start()

                @pl.when(inner & (m > 1))
                def _():
                    pass_on(t, s, part, slot + m - 1, z_dev(1)).start()

            @pl.when(i < 6)
            def _():
                part = 2 * turn(r + 1) + c
                arrive(t, sp, part)
                onward(sp, part, r + 1, 28)
                pass_on(t, sp, part, 5 + r, x_dev).start()
                pass_on(t, sp, part, 9 + r, y_dev).start()
                pass_on(t, sp, part, 1 + r, partner).start()

            @pl.when(i < 8)
            def _():
                part = 2 * turn(r) + c
                even = lax.rem(r, 2) == 0
                arrive(t, xn, part)

                @pl.when(even & (t == 0))
                def _():
                    pass_on(t, xn, part, 31 + r, y_dev).start()

                @pl.when((r == 0) & (t == 1))
                def _():
                    pass_half(xn, part, 0, 31, y_dev).start()

                pass_on(t, xn, part, 15 + r, partner).start()
                arrive(t, yn, part)

                @pl.when((lax.rem(r, 2) == 1) & (t == 0))
                def _():
                    pass_on(t, yn, part, 31 + r, x_dev).start()

                @pl.when((r == 0) & (t == 1))
                def _():
                    pass_half(yn, part, 1, 32, x_dev).start()

                pass_on(t, yn, part, 19 + r, partner).start()

            @pl.when((i >= 2) & (i < 10))
            def _():
                m = r - 1
                part = 2 * turn(m) + c
                arrive(t, dn, part)

                @pl.when((t == 1) & (m == 0))
                def _():
                    pass_on(t, dn, part, 35, z_dev(1)).start()

                    @pl.when(inner)
                    def _():
                        pass_on(t, dn, part, 36, z_dev(3)).start()

                @pl.when((t == 1) & (m > 0))
                def _():
                    onward(dn, part, m, 37)

                pass_on(t, dn, part, 22 + r, partner).start()

            @pl.when(i == 2)
            def _():
                close_edges(ci, ci_edges)
                conv[...] = (
                    ci[pl.ds(pad - 1, tokens), :] * taps[0:1, :]
                    + ci[middle, :] * taps[1:2, :]
                    + ci[pl.ds(pad + 1, tokens), :] * taps[2:3, :]
                )
                mixed[sp] = (gates[0].astype(jnp.float32) * conv[...]).astype(jnp.bfloat16)

            @pl.when(i >= 3)
            def _():
                j = i - 3
                kj, tj = (lax.div(j, 2), lax.rem(j, 2))
                layer = turn(kj)
                for s in range(groups):
                    arrive(tj, s, 2 * layer + near)
                multiply(tj, layer)

            return carry

        lax.fori_loop(0, 11, step, 0)

        for copy in route_copies:
            copy.wait()
        for copy in weight_copies:
            copy.wait()
        half = 128
        eye = lax.broadcasted_iota(jnp.int32, (half, half), 0) == lax.broadcasted_iota(
            jnp.int32, (half, half), 1
        )
        a_copies = []

        def gate_rows(i, s):
            columns = []
            for h in range(tokens // half):
                line = jnp.broadcast_to(wrow[s, 0:1, h * half : (h + 1) * half], (half, half))
                columns.append(jnp.sum(jnp.where(eye, line, 0.0), axis=1, keepdims=True))

            for h in range(tokens // half):
                start = pl.multiple_of(s * tokens + h * half, half)
                here = pl.ds(start, half)
                gate, up = (acc[here, pl.ds(0, hidden)], acc[here, pl.ds(hidden, hidden)])
                back = acc_down[here, :] * columns[h]
                sig = jax.nn.sigmoid(gate)
                act = gate * sig
                a[here, pl.ds(0, hidden)] = (back * up * sig * (1.0 + gate * (1.0 - sig))).astype(jnp.bfloat16)
                a[here, pl.ds(hidden, hidden)] = (back * act).astype(jnp.bfloat16)
                ht[:, pl.ds(start, half)] = (act * up * columns[h]).T.astype(jnp.bfloat16)
            copy = remote(a.at[rows(s)], a_far.at[rows(s)], a_send.at[i], a_recv.at[i], partner)
            copy.start()
            a_copies.append(copy)

        def weight_copy(j, slot, part):
            target = (gg_out, gu_out)[j]
            return pltpu.make_async_copy(stage.at[slot, j], target.at[part], st_sem.at[slot, j])

        def down_copy(part):
            cols = pl.ds(pl.multiple_of(part * width, width), width)
            return pltpu.make_async_copy(wd.at[part], gd_out.at[:, cols], gd_sem.at[part])

        def weight_grads(first, stop):
            tile = 256

            @pl.loop(first, stop)
            def _(part):
                slot = lax.rem(part, 2)

                @pl.when(part >= 2)
                def _():
                    for j in (0, 1):
                        weight_copy(j, slot, part).wait()

                @pl.loop(0, width // tile)
                def _(n):
                    feats = pl.ds(pl.multiple_of(n * tile, tile), tile)
                    totals = [0.0, 0.0]
                    for g in range(groups):
                        here = pl.ds(g * tokens, tokens)
                        turned = xc[0, part, here, feats].T
                        for j in (0, 1):
                            totals[j] += dot_nn(turned, a[here, pl.ds(j * hidden, hidden)])
                    for j in (0, 1):
                        stage[slot, j, feats, :] = totals[j].astype(jnp.bfloat16)

                    wd[part, :, feats] = dot_nn(ht[...], xc[1, part, :, feats]).astype(jnp.bfloat16)

                for j in (0, 1):
                    weight_copy(j, slot, part).start()
                down_copy(part).start()

        chunks = 4
        span = tokens // chunks

        def part_rows(q):
            return pl.ds(pl.multiple_of(q * span, span), span)

        def partial(s, k, finish):
            layer = flip(z, k)
            value = dot_nt(a[rows(s), :], w[2 * layer + c]) + dot_nt(a_far[rows(s), :], wp[layer])
            finish[k] = value.astype(finish.dtype)

        def rs_copy(kind, k, q, device):
            source, target = ((sd, rd), (sx, rx), (sy, ry))[kind]
            return remote(
                source.at[k, part_rows(q)],
                target.at[k, part_rows(q)],
                rs_send.at[kind, k, q],
                rs_recv.at[kind, k, q],
                device,
            )

        def landed(kind, k, q):
            rs_copy(kind, k, q, partner).wait_recv()

        def wide(ref):
            return ref.astype(jnp.float32)

        def merge(kind, k, q):
            landed(0, k, q)
            here = part_rows(q)
            buffer = (None, sx, sy)[kind]
            buffer[k, here, :] = (wide(buffer[k, here, :]) + wide(rd[k, here, :])).astype(jnp.bfloat16)
            rs_copy(kind, k, q, (None, x_dev, y_dev)[kind]).start()

        def stage_a(q):
            rs_copy(0, 2, q, x_dev).start()
            rs_copy(0, 3, q, y_dev).start()
            rs_copy(1, 2, q, x_dev).start()
            rs_copy(2, 3, q, y_dev).start()
            rs_copy(0, 0, q, x_dev).start()
            rs_copy(0, 1, q, y_dev).start()

        def stage_b(q):
            merge(2, 2, q)
            merge(1, 3, q)
            rs_copy(1, 0, q, x_dev).start()
            rs_copy(2, 1, q, y_dev).start()

        def stage_c(q):
            merge(2, 0, q)
            merge(1, 1, q)

        def z_ship(k, q):
            straight = lax.div(q, chunks - 1)
            hop = 1 if k == 1 else (1 + 2 * mid) * (1 - straight) + k * straight
            to = flip(z, hop)
            slot = {1: 0, 2: 3 + 2 * mid, 3: 2 + 2 * mid}[k] * (1 - straight) + k * straight
            return remote(
                sz.at[k, part_rows(q)],
                rz.at[slot, part_rows(q)],
                z_send.at[k, q],
                z_recv.at[slot, q],
                (sp, 2 * to + c),
            )

        def z_landed(slot, q):
            remote(
                sz.at[0, part_rows(q)], rz.at[slot, part_rows(q)], z_send.at[0, q], z_recv.at[slot, q], partner
            ).wait_recv()

        def collect(k, q):
            landed(1, k, q)
            landed(2, k, q)
            here = part_rows(q)
            total = sums[k, here, :] + wide(rx[k, here, :]) + wide(ry[k, here, :])
            sums[k, here, :] = total
            if k:

                @pl.when((mid == 0) | (q == chunks - 1))
                def _():
                    sz[k, here, :] = total.astype(jnp.bfloat16)
                    z_ship(k, q).start()

        def pass_along(k, q):
            here = part_rows(q)
            slot = {1: 5, 2: 2, 3: 3}[k]

            @pl.when(inner)
            def _():
                z_landed(slot, q)
                total = sums[k, here, :] + wide(rz[slot, here, :])
                sz[k, here, :] = total.astype(jnp.bfloat16)
                z_ship(k, q).start()

        def m_copy(q, part, slot, device):
            return remote(
                m.at[part, part_rows(q)],
                m.at[part, part_rows(q)],
                m_send.at[q, slot],
                m_recv.at[q, part],
                device,
            )

        def conclude(q):
            here = part_rows(q)
            mine = pl.ds(pl.multiple_of(sp * tokens + q * span, span), span)

            @pl.when(q < chunks - 1)
            def _():
                z_landed(0, q)

                @pl.when(inner)
                def _():
                    z_landed(4, q)

                total = sums[0, here, :] + wide(xc[1, tp, mine, :])
                total += wide(rz[0, here, :]) + wide(rz[4, here, :])
                m[tp, here, :] = total.astype(jnp.bfloat16)

            @pl.when(q == chunks - 1)
            def _():
                total = sums[0, here, :] + wide(xc[1, tp, mine, :])
                for k in (1, 2, 3):
                    z_landed(k, q)
                    total += wide(rz[k, here, :])
                m[tp, here, :] = total.astype(jnp.bfloat16)

            for k in (3, 2, 1):
                m_copy(q, tp, k, z_dev(k)).start()
            m_copy(q, tp, 0, partner).start()

        def across(q, k):
            layer = flip(z, k)
            return layer != sp, remote(
                m.at[2 * layer + c, part_rows(q)],
                cols_in.at[sp, c, part_rows(q)],
                a2_send.at[q, k],
                a2_recv.at[q, sp],
                (layer, tp),
            )

        def beside(q, s, side):
            return remote(
                cols_in.at[s, side, part_rows(q)],
                cols_in.at[s, side, part_rows(q)],
                a2p_send.at[q, s],
                a2p_recv.at[q, s],
                partner,
            )

        def spread(q):
            for k in (0, 3, 2, 1):
                part = 2 * flip(z, k) + c
                if k:
                    m_copy(q, part, 0, partner).wait_recv()
                    m_copy(q, part, 3 + k, partner).start()
                needed, copy = across(q, k)

                @pl.when(needed)
                def _():
                    copy.start()

        def project(q):
            here = part_rows(q)
            for layer in range(layers):
                m_copy(q, 2 * layer + near, 0, partner).wait_recv()
            total = dot_nn(m[0, here, :], op[0])
            for part in range(1, parts):
                total += dot_nn(m[part, here, :], op[part])
            gm[here, :] = total

        def relay(q):
            for d in (1, 2, 3):
                s = lax.rem(sp + d, groups)
                remote(
                    m.at[tp, part_rows(q)], cols_in.at[s, c, part_rows(q)], a2_send.at[q, 0], a2_recv.at[q, s], partner
                ).wait_recv()
                beside(q, s, c).start()

        def partner_rows(i):
            a_copies[i].wait_recv()

        gate_rows(0, dn)
        gate_rows(1, xn)
        partner_rows(0)
        partial(dn, 2, sd)
        rs_copy(0, 2, 0, x_dev).start()
        partial(dn, 3, sd)
        rs_copy(0, 3, 0, y_dev).start()
        gate_rows(2, yn)
        partner_rows(1)
        partial(xn, 2, sx)
        rs_copy(1, 2, 0, x_dev).start()
        gate_rows(3, sp)
        partner_rows(2)
        partial(yn, 3, sy)
        rs_copy(2, 3, 0, y_dev).start()
        partial(dn, 0, sd)
        rs_copy(0, 0, 0, x_dev).start()
        partial(dn, 1, sd)
        rs_copy(0, 1, 0, y_dev).start()
        stage_a(1)
        partner_rows(3)
        partial(yn, 2, sy)
        partial(xn, 3, sx)
        partial(xn, 0, sx)
        partial(yn, 1, sy)
        mixed_copies = [
            remote(mixed.at[sp], mixed.at[sp], mx_send.at[i], mx_recv.at[sp], device)
            for i, device in enumerate((x_dev, y_dev, d_dev))
        ]

        def during(q, first, last, work):
            @pl.when((q >= first) & (q <= last))
            def _():
                work(q - first)

        last = chunks - 1
        stage_b(0)
        partial(yn, 0, sy)
        partial(xn, 1, sx)
        stage_c(0)
        stage_a(2)
        for k in (3, 2, 1, 0):
            partial(sp, k, sums)

        def merge_next(i):
            stage_b(i + 1)
            stage_c(i + 1)

            @pl.when(i + 3 <= last)
            def _():
                stage_a(i + 3)

            @pl.when(i + 1 == last)
            def _():
                for copy in mixed_copies:
                    copy.start()

        def far_collect(i):
            collect(3, i)
            collect(2, i)

        def near_collect(i):
            collect(1, i)
            collect(0, i)

        def handed(i):
            pass_along(2, i)
            pass_along(3, i)

        def spare(i):
            project(i)
            relay(i)

        def round_trip(q, carry):
            during(q, 1, chunks - 1, lambda i: pass_along(1, i))
            during(q, 0, last - 1, merge_next)
            during(q, 0, last, lambda i: weight_grads(2 * i, 2 * i + 1))
            during(q, 0, last, far_collect)
            during(q, 1, chunks, conclude)
            during(q, 2, chunks + 1, spread)
            during(q, 0, last, near_collect)
            during(q, 0, last - 1, handed)
            during(q, 0, last, lambda i: weight_grads(2 * i + 1, 2 * i + 2))
            during(q, 3, chunks + 1, spare)
            return carry

        op_load.wait()
        lax.fori_loop(0, chunks + 2, round_trip, 0)
        project(last)
        gc[middle, :] = gm[...] * gates[0].astype(jnp.float32)
        gc_edges = edges(gc, 1)
        for copy in gc_edges:
            copy.start()
        outs_v[0] = (gm[...] * conv[...]).astype(jnp.bfloat16)
        finals = [pltpu.make_async_copy(outs_v.at[0], gog_out, out_sem.at[3])]
        finals[0].start()
        relay(last)
        for s in (xn, yn, dn):
            remote(mixed.at[s], mixed.at[s], mx_send.at[0], mx_recv.at[s], partner).wait_recv()

        tile = width // 2

        def out_side(side):
            here = pl.ds(pl.multiple_of(side * width, width), width)
            return pltpu.make_async_copy(acc.at[here], gop_out.at[here], out_sem.at[4 + side])

        @pl.loop(0, 2)
        def _(turn_of):
            side = lax.rem(c + turn_of, 2)

            @pl.when(turn_of == 1)
            def _():
                @pl.loop(0, chunks)
                def _(q):
                    for d in (1, 2, 3):
                        beside(q, lax.rem(sp + d, groups), near).wait_recv()

            @pl.loop(0, 2)
            def _(n):
                feats = pl.ds(pl.multiple_of(n * tile, tile), tile)
                total = dot_nn(m[2 * sp + side, :, feats].T, mixed[sp])
                for d in (1, 2, 3):
                    s = lax.rem(sp + d, groups)
                    total += dot_nn(cols_in[s, side, :, feats].T, mixed[s])
                acc[pl.ds(pl.multiple_of(side * width + n * tile, tile), tile), :] = total

            out_side(side).start()

        finals += [out_side(0), out_side(1)]
        close_edges(gc, gc_edges)
        grad = (
            gc[pl.ds(pad + 1, tokens), :] * taps[0:1, :]
            + gc[middle, :] * taps[1:2, :]
            + gc[pl.ds(pad - 1, tokens), :] * taps[2:3, :]
        )
        outs_v[1] = (grad * gates[2].astype(jnp.float32)).astype(jnp.bfloat16)
        outs_v[2] = (grad * gates[1].astype(jnp.float32)).astype(jnp.bfloat16)
        for j, target in ((1, gig_out), (2, gva_out)):
            copy = pltpu.make_async_copy(outs_v.at[j], target, out_sem.at[5 + j])
            copy.start()
            finals.append(copy)
        for copy in a_copies + mixed_copies + ci_edges + gc_edges:
            copy.wait_send()

        @pl.loop(0, chunks)
        def _(q):
            for kind, ks in ((0, range(4)), (1, range(4)), (2, range(4))):
                for k in ks:
                    rs_copy(kind, k, q, partner).wait_send()
            for slot in range(7):
                m_copy(q, tp, slot, partner).wait_send()
            for k in (1, 2, 3):
                z_ship(k, q).wait_send()
            for k in range(4):
                needed, copy = across(q, k)

                @pl.when(needed)
                def _():
                    copy.wait_send()

            for d in (1, 2, 3):
                beside(q, lax.rem(sp + d, groups), c).wait_send()

        for t in (0, 1):

            def sent(slot):
                pass_on(t, sp, tp, slot, partner).wait_send()

            pl.loop(0, 13)(sent)
            pl.loop(15, 27)(sent)
            if t:
                pass_half(sp, tp, 0, 31, partner).wait_send()
                pass_half(sp, tp, 0, 32, partner).wait_send()
                sent(35)
            else:
                pl.loop(31, 35)(sent)

            @pl.when(inner)
            def _():
                sent(13)
                pl.loop(28, 31)(sent)
                if t:
                    pl.loop(36, 40)(sent)

        for slot in (0, 1):
            for j in (0, 1):
                weight_copy(j, slot, slot).wait()
        for part in range(parts):
            down_copy(part).wait()
        for copy in finals:
            copy.wait()

    block_shape = (layers, tokens, width)
    shapes = [
        jax.ShapeDtypeStruct((parts, width, hidden), jnp.bfloat16),
        jax.ShapeDtypeStruct((parts, width, hidden), jnp.bfloat16),
        jax.ShapeDtypeStruct((hidden, parts * width), jnp.bfloat16),
    ]
    shapes += [jax.ShapeDtypeStruct((tokens, width), jnp.bfloat16)] * 3
    shapes.append(jax.ShapeDtypeStruct((2 * width, width), jnp.float32))
    half = jnp.bfloat16
    return pl.pallas_call(
        kernel,
        out_shape=shapes,
        in_specs=[pl.BlockSpec(memory_space=pl.ANY)] * 9
        + [pl.BlockSpec(memory_space=pltpu.VMEM), pl.BlockSpec(memory_space=pl.ANY)],
        out_specs=[pl.BlockSpec(memory_space=pl.ANY)] * 7,
        scratch_shapes=[
            pltpu.VMEM((2, parts, rows_all, width), half),
            pltpu.VMEM((parts, width, 2 * hidden), half),
            pltpu.VMEM((parts, hidden, width), half),
            pltpu.VMEM((layers, width, 2 * hidden), half),
            pltpu.VMEM((rows_all, 2 * hidden), jnp.float32),
            pltpu.VMEM((rows_all, hidden), jnp.float32),
            pltpu.VMEM((rows_all, 2 * hidden), half),
            pltpu.VMEM((rows_all, 2 * hidden), half),
            pltpu.VMEM((hidden, rows_all), half),
            pltpu.VMEM((2, 2, width, hidden), half),
            pltpu.VMEM((groups, 8, tokens), jnp.float32),
            pltpu.VMEM(block_shape, jnp.float32),
        ]
        + [pltpu.VMEM(block_shape, half)] * 7
        + [
            pltpu.VMEM((6, tokens, width), half),
            pltpu.VMEM((parts, width, width), half),
            pltpu.VMEM((parts, tokens, width), half),
            pltpu.VMEM((groups, 2, tokens, width), half),
            pltpu.VMEM((groups, tokens, width), half),
            pltpu.VMEM((tokens + 16, width), jnp.float32),
            pltpu.VMEM((tokens + 16, width), jnp.float32),
            pltpu.VMEM((tokens, width), jnp.float32),
            pltpu.VMEM((tokens, width), jnp.float32),
            pltpu.VMEM((3, tokens, width), half),
            pltpu.VMEM((3, tokens, width), half),
            pltpu.SemaphoreType.DMA((9 + parts,)),
            pltpu.SemaphoreType.DMA((2, 40)),
            pltpu.SemaphoreType.DMA((2, groups, parts)),
            pltpu.SemaphoreType.DMA((3,)),
            pltpu.SemaphoreType.DMA((3,)),
            pltpu.SemaphoreType.DMA((layers,)),
            pltpu.SemaphoreType.DMA((layers,)),
            pltpu.SemaphoreType.DMA((groups,)),
            pltpu.SemaphoreType.DMA((groups,)),
            pltpu.SemaphoreType.DMA((3, layers, 4)),
            pltpu.SemaphoreType.DMA((3, layers, 4)),
            pltpu.SemaphoreType.DMA((layers, 4)),
            pltpu.SemaphoreType.DMA((6, 4)),
            pltpu.SemaphoreType.DMA((8,)),
            pltpu.SemaphoreType.DMA((2, 2)),
            pltpu.SemaphoreType.DMA((parts,)),
            pltpu.SemaphoreType.DMA((2, 2)),
            pltpu.SemaphoreType.DMA((2, 2)),
            pltpu.SemaphoreType.DMA((3,)),
            pltpu.SemaphoreType.DMA((groups,)),
            pltpu.SemaphoreType.DMA((4, 7)),
            pltpu.SemaphoreType.DMA((4, parts)),
            pltpu.SemaphoreType.DMA((4, layers)),
            pltpu.SemaphoreType.DMA((4, groups)),
            pltpu.SemaphoreType.DMA((4, groups)),
            pltpu.SemaphoreType.DMA((4, groups)),
        ],
        compiler_params=pltpu.CompilerParams(
            collective_id=10, has_side_effects=True, vmem_limit_bytes=62 * 1024 * 1024
        ),
    )


def finish(grads, rest):
    pieces = 4
    count, total = (len(grads), len(grads) + len(rest))

    def kernel(*refs):
        sources, targets = (refs[:total], refs[total : 2 * total])
        narrow, broad = (refs[2 * total : 2 * total + count], refs[2 * total + count : 2 * total + 2 * count])
        through = refs[2 * total + 2 * count : 3 * total + count]
        in_sem, out_sem = refs[-2:]

        def piece(ref, i):
            size = ref.shape[0] // pieces
            return ref.at[pl.ds(i * size, size)]

        fetches = {}
        for i in range(pieces):
            for j in range(count):
                fetches[i, j] = pltpu.make_async_copy(
                    piece(sources[j], i), piece(narrow[j], i), in_sem.at[j, i]
                )
                fetches[i, j].start()
        for j in range(count, total):
            fetches[0, j] = pltpu.make_async_copy(sources[j], through[j - count], in_sem.at[j, 0])
            fetches[0, j].start()
        stores = []

        def store(source, target, j, i):
            copy = pltpu.make_async_copy(source, target, out_sem.at[j, i])
            copy.start()
            stores.append(copy)

        for i in range(pieces):
            for j in range(count):
                fetches[i, j].wait()
                size = narrow[j].shape[0] // pieces
                steps = 4
                rows = size // steps

                @pl.loop(0, steps)
                def _(n):
                    here = pl.ds(pl.multiple_of(i * size + n * rows, rows), rows)
                    broad[j][here, :] = narrow[j][here, :].astype(jnp.float32)

                store(piece(broad[j], i), piece(targets[j], i), j, i)
        for j in range(count, total):
            fetches[0, j].wait()
            store(through[j - count], targets[j], j, 0)
        for copy in stores:
            copy.wait()

    shapes = [jax.ShapeDtypeStruct(g.shape, jnp.float32) for g in grads]
    shapes += [jax.ShapeDtypeStruct(r.shape, r.dtype) for r in rest]
    return pl.pallas_call(
        kernel,
        out_shape=shapes,
        in_specs=[pl.BlockSpec(memory_space=pl.ANY)] * total,
        out_specs=[pl.BlockSpec(memory_space=pl.ANY)] * total,
        scratch_shapes=[pltpu.VMEM(g.shape, g.dtype) for g in grads]
        + [pltpu.VMEM(g.shape, jnp.float32) for g in grads]
        + [pltpu.VMEM(r.shape, r.dtype) for r in rest]
        + [pltpu.SemaphoreType.DMA((total, pieces))] * 2,
        compiler_params=pltpu.CompilerParams(vmem_limit_bytes=62 * 1024 * 1024),
    )(*grads, *rest)


def near_body(
    moe_input,
    out_gate,
    in_gate,
    values,
    conv_taps,
    out_proj,
    route_ids,
    route_gates,
    expert_gate,
    expert_up,
    expert_down,
    cotangent,
):
    token_count, part_width = moe_input.shape
    group_count = lax.axis_size("sp")
    hidden = expert_gate.shape[2]
    part_count = lax.axis_size("tp")
    shape = (group_count, 8, token_count)
    expert = lax.broadcasted_iota(jnp.int32, shape, 0)
    route = jnp.zeros(shape, jnp.float32)
    for pick in range(route_ids.shape[1]):
        chosen = route_ids[:, pick][None, None, :] == expert
        route += jnp.where(chosen, route_gates[:, pick][None, None, :], 0.0)
    (
        grad_expert_gate,
        grad_expert_up,
        grad_expert_down,
        grad_out_gate,
        grad_in_gate,
        grad_values,
        grad_out_proj,
    ) = experts_kernel(token_count, part_width, hidden)(
        moe_input,
        cotangent,
        route,
        expert_gate.reshape(part_count, part_width, hidden),
        expert_up.reshape(part_count, part_width, hidden),
        expert_down[0],
        out_gate,
        in_gate,
        values,
        conv_taps,
        out_proj.reshape(part_count, part_width, part_width),
    )

    (
        grad_expert_gate,
        grad_expert_up,
        grad_expert_down,
        grad_out_gate,
        grad_in_gate,
        grad_values,
        grad_out_proj,
    ) = finish(
        (
            grad_expert_gate.reshape(-1, hidden),
            grad_expert_up.reshape(-1, hidden),
            grad_expert_down,
        ),
        (grad_out_gate, grad_in_gate, grad_values, grad_out_proj),
    )
    grad_expert_gate = grad_expert_gate[None]
    grad_expert_up = grad_expert_up[None]
    grad_expert_down = grad_expert_down[None]
    return (
        grad_out_gate,
        grad_in_gate,
        grad_values,
        grad_out_proj,
        grad_expert_gate,
        grad_expert_up,
        grad_expert_down,
    )


def step(*arrays):
    moe_input, expert_gate, out_proj = (arrays[0], arrays[8], arrays[5])
    tokens, width = moe_input.shape
    near = (
        lax.axis_size("sp") == 4
        and lax.axis_size("tp") == 8
        and expert_gate.shape[0] == 1
        and tokens % 256 == 0
        and width == 2 * expert_gate.shape[2] == 2 * tokens
        and out_proj.shape[0] == 8 * width
    )
    return (near_body if near else body)(*arrays)


def solution(mesh):
    return jax.shard_map(
        step,
        mesh=mesh,
        in_specs=(
            P("sp", "tp"),
            P("sp", "tp"),
            P("sp", "tp"),
            P("sp", "tp"),
            P(None, "tp"),
            P(None, "tp"),
            P("sp", None),
            P("sp", None),
            P("sp", None, "tp"),
            P("sp", None, "tp"),
            P("sp", "tp", None),
            P("sp", "tp"),
        ),
        out_specs=(
            P("sp", "tp"),
            P("sp", "tp"),
            P("sp", "tp"),
            P("sp", "tp"),
            P("sp", None, "tp"),
            P("sp", None, "tp"),
            P("sp", "tp", None),
        ),
        check_vma=False,
    )
```

```python
import jax
import jax.numpy as jnp
from jax import lax
from jax.experimental import pallas as pl
from jax.experimental.pallas import tpu as pltpu
from jax.sharding import PartitionSpec as P

MESH = pl.DeviceIdType.MESH


def peers_of(group):
    sp, tp = (lax.axis_index("sp"), lax.axis_index("tp"))
    if group == "core":
        me, size = (lax.rem(tp, 2), 2)
    elif group == "z":
        me, size = (lax.div(tp, 2), lax.axis_size("tp") // 2)
    else:
        me, size = (sp, lax.axis_size("sp"))
    others = []
    for k in range(1, size):
        place = lax.rem(me + k, size)
        if group == "core":
            others.append((place, (sp, tp - me + place)))
        elif group == "z":
            others.append((place, (sp, place * 2 + lax.rem(tp, 2))))
        else:
            others.append((place, (place, tp)))
    return me, others


def group_size(group):
    if group == "core":
        return 2
    return lax.axis_size("tp") // 2 if group == "z" else lax.axis_size("sp")


def block(ref, place, width):
    return ref.at[:, pl.ds(pl.multiple_of(place * width, width), width)]


def exchange(collective_id, *ops):
    arrays = [op[2] for op in ops]
    shapes = []
    counts = []
    for kind, group, array, *rest in ops:
        size = group_size(group)
        if kind == "cores":
            shape, count = ((array.shape[0], array.shape[1] // 2), array.shape[1] // rest[0] // 2)
        elif kind == "columns":
            shape = (size - 1, array.shape[0], array.shape[1] // size)
            count = size - 1
        elif kind == "rows":
            shape, count = ((size - 1,) + array.shape[1:], size - 1)
        elif kind == "gather":
            shape, count = ((array.shape[0], array.shape[1] * size), size - 1)
        elif kind == "send":
            shape, count = (array.shape, size - 1)
        elif kind == "stack":
            shape, count = ((size,) + array.shape, size - 1)
        else:
            shape, count = (array.shape, 1)
        shapes.append(jax.ShapeDtypeStruct(shape, array.dtype))
        counts.append(count)
    total = sum(counts)

    def kernel(*refs):
        n = len(ops)
        sources, targets = (refs[:n], refs[n : 2 * n])
        send_sem, recv_sem, own_sem = refs[2 * n :]
        barrier = pltpu.get_barrier_semaphore()
        greeted = 0
        for group in sorted({op[1] for op in ops}):
            for _, device in peers_of(group)[1]:
                pl.semaphore_signal(barrier, inc=1, device_id=device, device_id_type=MESH)
                greeted += 1
        pl.semaphore_wait(barrier, greeted)
        copies = []
        local = []
        for i, (kind, group, array, *rest) in enumerate(ops):
            me, others = peers_of(group)
            source, target = (sources[i], targets[i])
            moves = []
            if kind == "cores":
                width = rest[0]
                place, device = others[0]
                for b in range(counts[i]):
                    moves.append(
                        (
                            block(source, 2 * b + place, width),
                            target.at[:, pl.ds(b * width, width)],
                            device,
                        )
                    )
            for k, (place, device) in enumerate(others):
                if kind == "columns":
                    moves.append((block(source, place, shapes[i].shape[2]), target.at[k], device))
                elif kind == "rows":
                    moves.append((source.at[place], target.at[k], device))
                elif kind == "gather":
                    moves.append((source, block(target, me, array.shape[1]), device))
                elif kind == "send":
                    moves.append((source.at[place], target.at[me], device))
                elif kind == "stack":
                    moves.append((source, target.at[me], device))
                elif kind == "swap":
                    moves.append((source, target, device))
            for a, b, device in moves:
                j = len(copies)
                copy = pltpu.make_async_remote_copy(
                    src_ref=a,
                    dst_ref=b,
                    send_sem=send_sem.at[j],
                    recv_sem=recv_sem.at[j],
                    device_id=device,
                    device_id_type=MESH,
                )
                copy.start()
                copies.append(copy)
            if kind == "gather":
                local.append((source, block(target, me, array.shape[1]), i))
            elif kind == "send":
                local.append((source.at[me], target.at[me], i))
            elif kind == "stack":
                local.append((source, target.at[me], i))
        own = [pltpu.make_async_copy(a, b, own_sem.at[i]) for a, b, i in local]
        for copy in own:
            copy.start()
        for copy in own + copies:
            copy.wait()

    return pl.pallas_call(
        kernel,
        out_shape=shapes,
        in_specs=[pl.BlockSpec(memory_space=pl.ANY)] * len(ops),
        out_specs=[pl.BlockSpec(memory_space=pl.ANY)] * len(ops),
        scratch_shapes=[
            pltpu.SemaphoreType.DMA((total,)),
            pltpu.SemaphoreType.DMA((total,)),
            pltpu.SemaphoreType.DMA((len(ops),)),
        ],
        compiler_params=pltpu.CompilerParams(collective_id=collective_id, has_side_effects=True),
    )(*arrays)


def halves(array, width):
    core = lax.rem(lax.axis_index("tp"), 2)
    blocks = [
        lax.dynamic_slice_in_dim(array, (start + core) * width, width, axis=1)
        for start in range(0, array.shape[1] // width, 2)
    ]
    return jnp.concatenate(blocks, axis=1)


def interleave(own, other, width):
    core = lax.rem(lax.axis_index("tp"), 2)
    first, second = (jnp.where(core == 0, own, other), jnp.where(core == 0, other, own))
    blocks = []
    for start in range(0, own.shape[1], width):
        blocks.append(first[:, start : start + width])
        blocks.append(second[:, start : start + width])
    return jnp.concatenate(blocks, axis=1)


def padded(array, sides, width):
    for axis, dim in sides:
        size, length = (lax.axis_size(axis), array.shape[dim])
        up = [(i, (i + 1) % size) for i in range(size - 1)]
        down = [(j, i) for i, j in up]
        last = lax.slice_in_dim(array, length - width, length, axis=dim)
        initial = lax.slice_in_dim(array, 0, width, axis=dim)
        before = lax.ppermute(last, axis, up)
        after = lax.ppermute(initial, axis, down)
        array = jnp.concatenate([before, array, after], axis=dim)
    return array


def body(
    moe_input,
    out_gate,
    in_gate,
    values,
    conv_taps,
    out_proj,
    route_ids,
    route_gates,
    expert_gate,
    expert_up,
    expert_down,
    cotangent,
):
    token_count = moe_input.shape[0]
    part_width = moe_input.shape[1]
    pick_count = route_ids.shape[1]
    group_count = lax.axis_size("sp")
    local_count = expert_gate.shape[0]
    expert_count = group_count * local_count
    capacity = 3 * token_count // expert_count
    contract_rows = (((0,), (0,)), ((), ()))
    flat_ids = route_ids.reshape(-1)
    one_hot = (flat_ids[:, None] == jnp.arange(expert_count, dtype=jnp.int32)[None, :]).astype(
        jnp.int32
    )
    earlier = jnp.cumsum(one_hot, axis=0) - one_hot
    position = jnp.sum(earlier * one_hot, axis=1)
    slot_index = flat_ids * capacity + position
    block_rows = local_count * capacity
    slots = jnp.arange(expert_count * capacity, dtype=jnp.int32)
    hits = slots[:, None, None] == slot_index.reshape(token_count, pick_count)[None, :, :]
    take = jnp.any(hits, axis=2).astype(jnp.bfloat16)
    slot_weight = jnp.sum(jnp.where(hits, route_gates[None, :, :], 0.0), axis=(1, 2))
    conv_in = in_gate.astype(jnp.float32) * values.astype(jnp.float32)
    rimmed = padded(conv_in, (("sp", 0),), 1)
    conv_out = rimmed[:-2] * conv_taps[0] + rimmed[1:-1] * conv_taps[1] + rimmed[2:] * conv_taps[2]
    mixed = (out_gate.astype(jnp.float32) * conv_out).astype(jnp.bfloat16)
    rows_z, mixed_all = exchange(4, ("gather", "z", moe_input), ("stack", "sp", mixed))
    half = rows_z.shape[1]
    send_rows = jnp.dot(take, rows_z, preferred_element_type=jnp.float32).astype(jnp.bfloat16)
    cot_z, recv_rows = exchange(
        5,
        ("gather", "z", cotangent),
        ("send", "sp", send_rows.reshape(group_count, block_rows, half)),
    )
    send_cot = (
        slot_weight[:, None] * jnp.dot(take, cot_z, preferred_element_type=jnp.float32)
    ).astype(jnp.bfloat16)
    recv_rows = recv_rows.reshape(group_count * block_rows, half)
    recv_cot, swap_rows = exchange(
        6,
        ("send", "sp", send_cot.reshape(group_count, block_rows, half)),
        ("swap", "core", recv_rows),
    )
    recv_cot = recv_cot.reshape(group_count * block_rows, half)
    (swap_cot,) = exchange(7, ("swap", "core", recv_cot))

    def by_expert(own, other):
        full = interleave(own, other, part_width)
        full = full.reshape(group_count, local_count, capacity, 2 * half)
        return jnp.swapaxes(full, 0, 1).reshape(local_count, group_count * capacity, 2 * half)

    full_rows = by_expert(recv_rows, swap_rows)
    full_cot = by_expert(recv_cot, swap_cot)
    pre_gate = jnp.einsum(
        "prd,pdf->prf", full_rows, expert_gate, preferred_element_type=jnp.float32
    )
    pre_up = jnp.einsum("prd,pdf->prf", full_rows, expert_up, preferred_element_type=jnp.float32)
    gate_sig = jax.nn.sigmoid(pre_gate)
    activated = pre_gate * gate_sig
    hidden_act = (activated * pre_up).astype(jnp.bfloat16)
    grad_expert_down = jnp.einsum(
        "prf,prd->pfd", hidden_act, full_cot, preferred_element_type=jnp.float32
    )
    grad_hidden = jnp.einsum(
        "prd,pfd->prf", full_cot, expert_down, preferred_element_type=jnp.float32
    )
    grad_pre_gate = (grad_hidden * pre_up * gate_sig * (1.0 + pre_gate * (1.0 - gate_sig))).astype(
        jnp.bfloat16
    )
    grad_pre_up = (grad_hidden * activated).astype(jnp.bfloat16)
    grad_expert_gate = jnp.einsum(
        "prd,prf->pdf", full_rows, grad_pre_gate, preferred_element_type=jnp.float32
    )
    grad_expert_up = jnp.einsum(
        "prd,prf->pdf", full_rows, grad_pre_up, preferred_element_type=jnp.float32
    )
    partial_grad = jnp.einsum(
        "prf,pdf->prd", grad_pre_gate, expert_gate, preferred_element_type=jnp.float32
    ) + jnp.einsum("prf,pdf->prd", grad_pre_up, expert_up, preferred_element_type=jnp.float32)
    me = lax.axis_index("sp")
    partial_rows = partial_grad.astype(jnp.bfloat16).reshape(local_count * group_count * capacity, -1)
    (other_core,) = exchange(1, ("cores", "core", partial_rows, part_width))
    chip_rows = (
        halves(partial_rows, part_width).astype(jnp.float32) + other_core.astype(jnp.float32)
    ).astype(jnp.bfloat16)
    chip_rows = jnp.swapaxes(
        chip_rows.reshape(local_count, group_count, capacity, half), 0, 1
    ).reshape(group_count, block_rows, half)
    (returned,) = exchange(2, ("rows", "sp", chip_rows))
    back = lax.rem(me - jnp.arange(group_count) + group_count, group_count)
    local_slots = jnp.arange(block_rows, dtype=jnp.int32)
    picks = jnp.sum(
        (slot_index.reshape(token_count, pick_count)[None, :, :, None])
        == (back[:, None] * block_rows + local_slots)[:, None, None, :],
        axis=2,
    ).astype(jnp.bfloat16)
    token_part = jnp.dot(
        picks[0],
        lax.dynamic_index_in_dim(chip_rows, me, 0, keepdims=False),
        preferred_element_type=jnp.float32,
    ) + jnp.einsum("kts,ksd->td", picks[1:], returned, preferred_element_type=jnp.float32)
    token_part = token_part.astype(jnp.bfloat16)
    (parts,) = exchange(3, ("columns", "z", token_part))
    own_part = lax.dynamic_slice_in_dim(
        token_part, lax.div(lax.axis_index("tp"), 2) * part_width, part_width, axis=1
    )
    moe_grad = own_part.astype(jnp.float32) + jnp.sum(parts.astype(jnp.float32), axis=0)
    mixer_cot = (cotangent.astype(jnp.float32) + moe_grad).astype(jnp.bfloat16)
    (mixer_z,) = exchange(8, ("gather", "z", mixer_cot))
    (mixer_other,) = exchange(9, ("swap", "core", mixer_z))
    full_mixer_cot = interleave(mixer_z, mixer_other, part_width)
    grad_mixed = jnp.dot(full_mixer_cot, out_proj, preferred_element_type=jnp.float32)
    grad_out_gate = (grad_mixed * conv_out).astype(jnp.bfloat16)
    grad_conv_out = grad_mixed * out_gate.astype(jnp.float32)
    rim_grad = padded(grad_conv_out, (("sp", 0),), 1)
    grad_conv_in = (
        rim_grad[2:] * conv_taps[0] + rim_grad[1:-1] * conv_taps[1] + rim_grad[:-2] * conv_taps[2]
    )
    grad_in_gate = (grad_conv_in * values.astype(jnp.float32)).astype(jnp.bfloat16)
    grad_values = (grad_conv_in * in_gate.astype(jnp.float32)).astype(jnp.bfloat16)
    columns = lax.all_to_all(full_mixer_cot, "sp", split_axis=1, concat_axis=0, tiled=True)
    grad_out_proj = lax.dot_general(
        columns,
        mixed_all.reshape(group_count * token_count, part_width),
        contract_rows,
        preferred_element_type=jnp.float32,
    )
    return (
        grad_out_gate,
        grad_in_gate,
        grad_values,
        grad_out_proj,
        grad_expert_gate,
        grad_expert_up,
        grad_expert_down,
    )


def flip(index, bits):
    high, low = (lax.div(index, 2), lax.rem(index, 2))
    bit_high, bit_low = (lax.div(bits, 2), lax.rem(bits, 2)) if not isinstance(bits, int) else (bits // 2, bits % 2)
    high = high + bit_high - 2 * high * bit_high
    low = low + bit_low - 2 * low * bit_low
    return 2 * high + low


def place():
    sp, tp = (lax.axis_index("sp"), lax.axis_index("tp"))
    return sp, lax.div(tp, 2), lax.rem(tp, 2)


def greet(devices):
    barrier = pltpu.get_barrier_semaphore()
    for device in devices:
        pl.semaphore_signal(barrier, inc=1, device_id=device, device_id_type=MESH)
    pl.semaphore_wait(barrier, len(devices))


def remote(source, target, send_sem, recv_sem, device):
    return pltpu.make_async_remote_copy(
        src_ref=source,
        dst_ref=target,
        send_sem=send_sem,
        recv_sem=recv_sem,
        device_id=device,
        device_id_type=MESH,
    )


def dot_nt(a, b):
    return lax.dot_general(a, b, (((1,), (1,)), ((), ())), preferred_element_type=jnp.float32)


def dot_nn(a, b):
    return jnp.dot(a, b, preferred_element_type=jnp.float32)


def dot_tn(a, b):
    return lax.dot_general(a, b, (((0,), (0,)), ((), ())), preferred_element_type=jnp.float32)


def experts_kernel(tokens, width, hidden):
    groups, layers = (4, 4)
    parts = 2 * layers
    rows_all = groups * tokens

    def kernel(
        x_hbm, c_hbm, route, wg_hbm, wu_hbm, wd_hbm, og_hbm, ig_hbm, va_hbm, taps, op_hbm,
        gg_out, gu_out, gd_out, gog_out, gig_out, gva_out, gop_out,
        xc, w, wd, wp, acc, acc_down, a, a_far, ht, stage, wrow, sums,
        sd, sx, sy, sz, rd, rx, ry, rz,
        op, m, cols_in, mixed, ci, gc, conv, gm, gates, outs_v,
        load, xc_send, xc_recv, wr_send, wr_recv, wp_send, wp_recv, a_send, a_recv,
        rs_send, rs_recv, z_send, z_recv, out_sem, st_sem, gd_sem,
        edge_send, edge_recv, mx_send, mx_recv, m_send, m_recv, a2_send, a2_recv, a2p_send, a2p_recv,
    ):
        sp, z, c = place()
        tp = 2 * z + c
        xn, yn, dn = (flip(sp, 1), flip(sp, 2), flip(sp, 3))
        near = 1 - c
        partner = (sp, 2 * z + near)
        x_dev, y_dev, d_dev = ((xn, tp), (yn, tp), (dn, tp))

        mid = lax.rem(lax.div(z, 2) + lax.rem(z, 2), 2)
        inner = mid == 1

        def z_dev(k):
            return (sp, 2 * flip(z, k) + c)

        def rows(s):
            return pl.ds(pl.multiple_of(s * tokens, tokens), tokens)

        def blk(t, s, part):
            return xc.at[t, part, rows(s)]

        loads = [
            pltpu.make_async_copy(x_hbm, blk(0, sp, tp), load.at[0]),
            pltpu.make_async_copy(c_hbm, blk(1, sp, tp), load.at[1]),
            pltpu.make_async_copy(wg_hbm, w.at[:, :, pl.ds(0, hidden)], load.at[2]),
            pltpu.make_async_copy(wu_hbm, w.at[:, :, pl.ds(hidden, hidden)], load.at[3]),
            pltpu.make_async_copy(route.at[sp], wrow.at[sp], load.at[4]),
        ]
        for part in range(parts):
            loads.append(
                pltpu.make_async_copy(
                    wd_hbm.at[:, pl.ds(part * width, width)], wd.at[part], load.at[5 + part]
                )
            )
        conv_loads = [
            pltpu.make_async_copy(source, gates.at[j], load.at[5 + parts + j])
            for j, source in enumerate((og_hbm, ig_hbm, va_hbm))
        ]
        op_load = pltpu.make_async_copy(op_hbm, op, load.at[8 + parts])
        for copy in loads[:2]:
            copy.start()
        pad = 8
        middle = pl.ds(pad, tokens)

        def edges(buffer, phase):
            before, after = (lax.rem(sp + groups - 1, groups), lax.rem(sp + 1, groups))
            top, low = (pl.ds(0, pad), pl.ds(pad + tokens, pad))
            first, final = (pl.ds(pad, pad), pl.ds(tokens, pad))
            return [
                remote(
                    buffer.at[final], buffer.at[top], edge_send.at[phase, 0], edge_recv.at[phase, 0], (after, tp)
                ),
                remote(
                    buffer.at[first], buffer.at[low], edge_send.at[phase, 1], edge_recv.at[phase, 1], (before, tp)
                ),
            ]

        def close_edges(buffer, copies):
            for copy in copies:
                copy.wait_recv()

            @pl.when(sp == 0)
            def _():
                buffer[pl.ds(0, pad), :] = jnp.zeros((pad, width), jnp.float32)

            @pl.when(sp == groups - 1)
            def _():
                buffer[pl.ds(pad + tokens, pad), :] = jnp.zeros((pad, width), jnp.float32)

        ci_edges = edges(ci, 0)
        greet([partner, z_dev(1), z_dev(2), z_dev(3), x_dev, y_dev, d_dev])
        loads[0].wait()
        loads[1].wait()

        def pass_on(t, s, part, slot, device):
            return remote(
                blk(t, s, part), blk(t, s, part), xc_send.at[t, slot], xc_recv.at[t, s, part], device
            )

        def pass_half(s, part, h, slot, device):
            here = pl.ds(pl.multiple_of(s * tokens + h * (tokens // 2), tokens // 2), tokens // 2)
            block = xc.at[1, part, here]
            return remote(block, block, xc_send.at[1, slot], xc_recv.at[1, s, part], device)

        def arrive(t, s, part):
            pass_on(t, s, part, 0, partner).wait_recv()

        for t in (0, 1):
            pass_on(t, sp, tp, 12, z_dev(1)).start()

            @pl.when(inner)
            def _():
                pass_on(t, sp, tp, 13, z_dev(3)).start()

            pass_on(t, sp, tp, 4, x_dev).start()
            pass_on(t, sp, tp, 8, y_dev).start()
            pass_on(t, sp, tp, 0, partner).start()
        for copy in conv_loads + loads[2:] + [op_load]:
            copy.start()
        for copy in conv_loads:
            copy.wait()
        ci[middle, :] = gates[1].astype(jnp.float32) * gates[2].astype(jnp.float32)
        for copy in ci_edges:
            copy.start()
        route_copies = []
        for i, (s, device) in enumerate(((xn, x_dev), (yn, y_dev), (dn, d_dev))):
            copy = remote(route.at[s], wrow.at[sp], wr_send.at[i], wr_recv.at[i], device)
            copy.start()
            route_copies.append(copy)
        for copy in loads[2:]:
            copy.wait()
        weight_copies = []
        for part in range(layers):
            copy = remote(w.at[2 * part + near], wp.at[part], wp_send.at[part], wp_recv.at[part], partner)
            copy.start()
            weight_copies.append(copy)
        acc[...] = jnp.zeros_like(acc)
        acc_down[...] = jnp.zeros_like(acc_down)

        @pl.when(mid == 0)
        def _():
            rz[...] = jnp.zeros_like(rz)

        def multiply(t, layer):
            @pl.when(t == 0)
            def _():
                @pl.loop(0, groups)
                def _(s):
                    here = rows(s)
                    acc[here, :] += dot_nn(xc[0, 2 * layer, here, :], w[2 * layer]) + dot_nn(
                        xc[0, 2 * layer + 1, here, :], w[2 * layer + 1]
                    )

            @pl.when(t == 1)
            def _():
                @pl.loop(0, groups)
                def _(s):
                    here = rows(s)
                    acc_down[here, :] += dot_nt(xc[1, 2 * layer, here, :], wd[2 * layer]) + dot_nt(
                        xc[1, 2 * layer + 1, here, :], wd[2 * layer + 1]
                    )

        def turn(i):
            return flip(z, i + mid * lax.div(i, 2) * (5 - 2 * i))

        def step(i, carry):
            r, t = (lax.div(i, 2), lax.rem(i, 2))

            def onward(s, part, m, slot):
                @pl.when(inner & (m == 1))
                def _():
                    pass_on(t, s, part, slot, z_dev(3)).start()

                @pl.when(inner & (m > 1))
                def _():
                    pass_on(t, s, part, slot + m - 1, z_dev(1)).start()

            @pl.when(i < 6)
            def _():
                part = 2 * turn(r + 1) + c
                arrive(t, sp, part)
                onward(sp, part, r + 1, 28)
                pass_on(t, sp, part, 5 + r, x_dev).start()
                pass_on(t, sp, part, 9 + r, y_dev).start()
                pass_on(t, sp, part, 1 + r, partner).start()

            @pl.when(i < 8)
            def _():
                part = 2 * turn(r) + c
                even = lax.rem(r, 2) == 0
                arrive(t, xn, part)

                @pl.when(even & (t == 0))
                def _():
                    pass_on(t, xn, part, 31 + r, y_dev).start()

                @pl.when((r == 0) & (t == 1))
                def _():
                    pass_half(xn, part, 0, 31, y_dev).start()

                pass_on(t, xn, part, 15 + r, partner).start()
                arrive(t, yn, part)

                @pl.when((lax.rem(r, 2) == 1) & (t == 0))
                def _():
                    pass_on(t, yn, part, 31 + r, x_dev).start()

                @pl.when((r == 0) & (t == 1))
                def _():
                    pass_half(yn, part, 1, 32, x_dev).start()

                pass_on(t, yn, part, 19 + r, partner).start()

            @pl.when((i >= 2) & (i < 10))
            def _():
                m = r - 1
                part = 2 * turn(m) + c
                arrive(t, dn, part)

                @pl.when((t == 1) & (m == 0))
                def _():
                    pass_on(t, dn, part, 35, z_dev(1)).start()

                    @pl.when(inner)
                    def _():
                        pass_on(t, dn, part, 36, z_dev(3)).start()

                @pl.when((t == 1) & (m > 0))
                def _():
                    onward(dn, part, m, 37)

                pass_on(t, dn, part, 22 + r, partner).start()

            @pl.when(i == 2)
            def _():
                close_edges(ci, ci_edges)
                conv[...] = (
                    ci[pl.ds(pad - 1, tokens), :] * taps[0:1, :]
                    + ci[middle, :] * taps[1:2, :]
                    + ci[pl.ds(pad + 1, tokens), :] * taps[2:3, :]
                )
                mixed[sp] = (gates[0].astype(jnp.float32) * conv[...]).astype(jnp.bfloat16)

            @pl.when(i >= 3)
            def _():
                j = i - 3
                kj, tj = (lax.div(j, 2), lax.rem(j, 2))
                layer = turn(kj)
                for s in range(groups):
                    arrive(tj, s, 2 * layer + near)
                multiply(tj, layer)

            return carry

        lax.fori_loop(0, 11, step, 0)

        for copy in route_copies:
            copy.wait()
        for copy in weight_copies:
            copy.wait()
        half = 128
        eye = lax.broadcasted_iota(jnp.int32, (half, half), 0) == lax.broadcasted_iota(
            jnp.int32, (half, half), 1
        )
        a_copies = []

        def gate_rows(i, s):
            columns = []
            for h in range(tokens // half):
                line = jnp.broadcast_to(wrow[s, 0:1, h * half : (h + 1) * half], (half, half))
                columns.append(jnp.sum(jnp.where(eye, line, 0.0), axis=1, keepdims=True))

            for h in range(tokens // half):
                start = pl.multiple_of(s * tokens + h * half, half)
                here = pl.ds(start, half)
                gate, up = (acc[here, pl.ds(0, hidden)], acc[here, pl.ds(hidden, hidden)])
                back = acc_down[here, :] * columns[h]
                sig = jax.nn.sigmoid(gate)
                act = gate * sig
                a[here, pl.ds(0, hidden)] = (back * up * sig * (1.0 + gate * (1.0 - sig))).astype(jnp.bfloat16)
                a[here, pl.ds(hidden, hidden)] = (back * act).astype(jnp.bfloat16)
                ht[:, pl.ds(start, half)] = (act * up * columns[h]).T.astype(jnp.bfloat16)
            copy = remote(a.at[rows(s)], a_far.at[rows(s)], a_send.at[i], a_recv.at[i], partner)
            copy.start()
            a_copies.append(copy)

        def weight_copy(j, slot, part):
            target = (gg_out, gu_out)[j]
            return pltpu.make_async_copy(stage.at[slot, j], target.at[part], st_sem.at[slot, j])

        def down_copy(part):
            cols = pl.ds(pl.multiple_of(part * width, width), width)
            return pltpu.make_async_copy(wd.at[part], gd_out.at[:, cols], gd_sem.at[part])

        def weight_grads(first, stop):
            tile = 256

            @pl.loop(first, stop)
            def _(part):
                slot = lax.rem(part, 2)

                @pl.when(part >= 2)
                def _():
                    for j in (0, 1):
                        weight_copy(j, slot, part).wait()

                @pl.loop(0, width // tile)
                def _(n):
                    feats = pl.ds(pl.multiple_of(n * tile, tile), tile)
                    totals = [0.0, 0.0]
                    for g in range(groups):
                        here = pl.ds(g * tokens, tokens)
                        turned = xc[0, part, here, feats].T
                        for j in (0, 1):
                            totals[j] += dot_nn(turned, a[here, pl.ds(j * hidden, hidden)])
                    for j in (0, 1):
                        stage[slot, j, feats, :] = totals[j].astype(jnp.bfloat16)

                    wd[part, :, feats] = dot_nn(ht[...], xc[1, part, :, feats]).astype(jnp.bfloat16)

                for j in (0, 1):
                    weight_copy(j, slot, part).start()
                down_copy(part).start()

        chunks = 4
        span = tokens // chunks

        def part_rows(q):
            return pl.ds(pl.multiple_of(q * span, span), span)

        def partial(s, k, finish):
            layer = flip(z, k)
            value = dot_nt(a[rows(s), :], w[2 * layer + c]) + dot_nt(a_far[rows(s), :], wp[layer])
            finish[k] = value.astype(finish.dtype)

        def rs_copy(kind, k, q, device):
            source, target = ((sd, rd), (sx, rx), (sy, ry))[kind]
            return remote(
                source.at[k, part_rows(q)],
                target.at[k, part_rows(q)],
                rs_send.at[kind, k, q],
                rs_recv.at[kind, k, q],
                device,
            )

        def landed(kind, k, q):
            rs_copy(kind, k, q, partner).wait_recv()

        def wide(ref):
            return ref.astype(jnp.float32)

        def merge(kind, k, q):
            landed(0, k, q)
            here = part_rows(q)
            buffer = (None, sx, sy)[kind]
            buffer[k, here, :] = (wide(buffer[k, here, :]) + wide(rd[k, here, :])).astype(jnp.bfloat16)
            rs_copy(kind, k, q, (None, x_dev, y_dev)[kind]).start()

        def stage_a(q):
            rs_copy(0, 2, q, x_dev).start()
            rs_copy(0, 3, q, y_dev).start()
            rs_copy(1, 2, q, x_dev).start()
            rs_copy(2, 3, q, y_dev).start()
            rs_copy(0, 0, q, x_dev).start()
            rs_copy(0, 1, q, y_dev).start()

        def stage_b(q):
            merge(2, 2, q)
            merge(1, 3, q)
            rs_copy(1, 0, q, x_dev).start()
            rs_copy(2, 1, q, y_dev).start()

        def stage_c(q):
            merge(2, 0, q)
            merge(1, 1, q)

        def z_ship(k, q):
            straight = lax.div(q, chunks - 1)
            hop = 1 if k == 1 else (1 + 2 * mid) * (1 - straight) + k * straight
            to = flip(z, hop)
            slot = {1: 0, 2: 3 + 2 * mid, 3: 2 + 2 * mid}[k] * (1 - straight) + k * straight
            return remote(
                sz.at[k, part_rows(q)],
                rz.at[slot, part_rows(q)],
                z_send.at[k, q],
                z_recv.at[slot, q],
                (sp, 2 * to + c),
            )

        def z_landed(slot, q):
            remote(
                sz.at[0, part_rows(q)], rz.at[slot, part_rows(q)], z_send.at[0, q], z_recv.at[slot, q], partner
            ).wait_recv()

        def collect(k, q):
            landed(1, k, q)
            landed(2, k, q)
            here = part_rows(q)
            total = sums[k, here, :] + wide(rx[k, here, :]) + wide(ry[k, here, :])
            sums[k, here, :] = total
            if k:

                @pl.when((mid == 0) | (q == chunks - 1))
                def _():
                    sz[k, here, :] = total.astype(jnp.bfloat16)
                    z_ship(k, q).start()

        def pass_along(k, q):
            here = part_rows(q)
            slot = {1: 5, 2: 2, 3: 3}[k]

            @pl.when(inner)
            def _():
                z_landed(slot, q)
                total = sums[k, here, :] + wide(rz[slot, here, :])
                sz[k, here, :] = total.astype(jnp.bfloat16)
                z_ship(k, q).start()

        def m_copy(q, part, slot, device):
            return remote(
                m.at[part, part_rows(q)],
                m.at[part, part_rows(q)],
                m_send.at[q, slot],
                m_recv.at[q, part],
                device,
            )

        def conclude(q):
            here = part_rows(q)
            mine = pl.ds(pl.multiple_of(sp * tokens + q * span, span), span)

            @pl.when(q < chunks - 1)
            def _():
                z_landed(0, q)

                @pl.when(inner)
                def _():
                    z_landed(4, q)

                total = sums[0, here, :] + wide(xc[1, tp, mine, :])
                total += wide(rz[0, here, :]) + wide(rz[4, here, :])
                m[tp, here, :] = total.astype(jnp.bfloat16)

            @pl.when(q == chunks - 1)
            def _():
                total = sums[0, here, :] + wide(xc[1, tp, mine, :])
                for k in (1, 2, 3):
                    z_landed(k, q)
                    total += wide(rz[k, here, :])
                m[tp, here, :] = total.astype(jnp.bfloat16)

            for k in (3, 2, 1):
                m_copy(q, tp, k, z_dev(k)).start()
            m_copy(q, tp, 0, partner).start()

        def across(q, k):
            layer = flip(z, k)
            return layer != sp, remote(
                m.at[2 * layer + c, part_rows(q)],
                cols_in.at[sp, c, part_rows(q)],
                a2_send.at[q, k],
                a2_recv.at[q, sp],
                (layer, tp),
            )

        def beside(q, s, side):
            return remote(
                cols_in.at[s, side, part_rows(q)],
                cols_in.at[s, side, part_rows(q)],
                a2p_send.at[q, s],
                a2p_recv.at[q, s],
                partner,
            )

        def spread(q):
            for k in (0, 3, 2, 1):
                part = 2 * flip(z, k) + c
                if k:
                    m_copy(q, part, 0, partner).wait_recv()
                    m_copy(q, part, 3 + k, partner).start()
                needed, copy = across(q, k)

                @pl.when(needed)
                def _():
                    copy.start()

        def project(q):
            here = part_rows(q)
            for layer in range(layers):
                m_copy(q, 2 * layer + near, 0, partner).wait_recv()
            total = dot_nn(m[0, here, :], op[0])
            for part in range(1, parts):
                total += dot_nn(m[part, here, :], op[part])
            gm[here, :] = total

        def relay(q):
            for d in (1, 2, 3):
                s = lax.rem(sp + d, groups)
                remote(
                    m.at[tp, part_rows(q)], cols_in.at[s, c, part_rows(q)], a2_send.at[q, 0], a2_recv.at[q, s], partner
                ).wait_recv()
                beside(q, s, c).start()

        def partner_rows(i):
            a_copies[i].wait_recv()

        gate_rows(0, dn)
        gate_rows(1, xn)
        partner_rows(0)
        partial(dn, 2, sd)
        rs_copy(0, 2, 0, x_dev).start()
        partial(dn, 3, sd)
        rs_copy(0, 3, 0, y_dev).start()
        gate_rows(2, yn)
        partner_rows(1)
        partial(xn, 2, sx)
        rs_copy(1, 2, 0, x_dev).start()
        gate_rows(3, sp)
        partner_rows(2)
        partial(yn, 3, sy)
        rs_copy(2, 3, 0, y_dev).start()
        partial(dn, 0, sd)
        rs_copy(0, 0, 0, x_dev).start()
        partial(dn, 1, sd)
        rs_copy(0, 1, 0, y_dev).start()
        stage_a(1)
        partner_rows(3)
        partial(yn, 2, sy)
        partial(xn, 3, sx)
        partial(xn, 0, sx)
        partial(yn, 1, sy)
        mixed_copies = [
            remote(mixed.at[sp], mixed.at[sp], mx_send.at[i], mx_recv.at[sp], device)
            for i, device in enumerate((x_dev, y_dev, d_dev))
        ]

        def during(q, first, last, work):
            @pl.when((q >= first) & (q <= last))
            def _():
                work(q - first)

        last = chunks - 1
        stage_b(0)
        partial(yn, 0, sy)
        partial(xn, 1, sx)
        stage_c(0)
        stage_a(2)
        for k in (3, 2, 1, 0):
            partial(sp, k, sums)

        def merge_next(i):
            stage_b(i + 1)
            stage_c(i + 1)

            @pl.when(i + 3 <= last)
            def _():
                stage_a(i + 3)

            @pl.when(i + 1 == last)
            def _():
                for copy in mixed_copies:
                    copy.start()

        def far_collect(i):
            collect(3, i)
            collect(2, i)

        def near_collect(i):
            collect(1, i)
            collect(0, i)

        def handed(i):
            pass_along(2, i)
            pass_along(3, i)

        def spare(i):
            project(i)
            relay(i)

        def round_trip(q, carry):
            during(q, 1, chunks - 1, lambda i: pass_along(1, i))
            during(q, 0, last - 1, merge_next)
            during(q, 0, last, lambda i: weight_grads(2 * i, 2 * i + 1))
            during(q, 0, last, far_collect)
            during(q, 1, chunks, conclude)
            during(q, 2, chunks + 1, spread)
            during(q, 0, last, near_collect)
            during(q, 0, last - 1, handed)
            during(q, 0, last, lambda i: weight_grads(2 * i + 1, 2 * i + 2))
            during(q, 3, chunks + 1, spare)
            return carry

        op_load.wait()
        lax.fori_loop(0, chunks + 2, round_trip, 0)
        project(last)
        gc[middle, :] = gm[...] * gates[0].astype(jnp.float32)
        gc_edges = edges(gc, 1)
        for copy in gc_edges:
            copy.start()
        outs_v[0] = (gm[...] * conv[...]).astype(jnp.bfloat16)
        finals = [pltpu.make_async_copy(outs_v.at[0], gog_out, out_sem.at[3])]
        finals[0].start()
        relay(last)
        for s in (xn, yn, dn):
            remote(mixed.at[s], mixed.at[s], mx_send.at[0], mx_recv.at[s], partner).wait_recv()

        tile = width // 2

        def out_side(side):
            here = pl.ds(pl.multiple_of(side * width, width), width)
            return pltpu.make_async_copy(acc.at[here], gop_out.at[here], out_sem.at[4 + side])

        @pl.loop(0, 2)
        def _(turn_of):
            side = lax.rem(c + turn_of, 2)

            @pl.when(turn_of == 1)
            def _():
                @pl.loop(0, chunks)
                def _(q):
                    for d in (1, 2, 3):
                        beside(q, lax.rem(sp + d, groups), near).wait_recv()

            @pl.loop(0, 2)
            def _(n):
                feats = pl.ds(pl.multiple_of(n * tile, tile), tile)
                total = dot_nn(m[2 * sp + side, :, feats].T, mixed[sp])
                for d in (1, 2, 3):
                    s = lax.rem(sp + d, groups)
                    total += dot_nn(cols_in[s, side, :, feats].T, mixed[s])
                acc[pl.ds(pl.multiple_of(side * width + n * tile, tile), tile), :] = total

            out_side(side).start()

        finals += [out_side(0), out_side(1)]
        close_edges(gc, gc_edges)
        grad = (
            gc[pl.ds(pad + 1, tokens), :] * taps[0:1, :]
            + gc[middle, :] * taps[1:2, :]
            + gc[pl.ds(pad - 1, tokens), :] * taps[2:3, :]
        )
        outs_v[1] = (grad * gates[2].astype(jnp.float32)).astype(jnp.bfloat16)
        outs_v[2] = (grad * gates[1].astype(jnp.float32)).astype(jnp.bfloat16)
        for j, target in ((1, gig_out), (2, gva_out)):
            copy = pltpu.make_async_copy(outs_v.at[j], target, out_sem.at[5 + j])
            copy.start()
            finals.append(copy)
        for copy in a_copies + mixed_copies + ci_edges + gc_edges:
            copy.wait_send()

        @pl.loop(0, chunks)
        def _(q):
            for kind, ks in ((0, range(4)), (1, range(4)), (2, range(4))):
                for k in ks:
                    rs_copy(kind, k, q, partner).wait_send()
            for slot in range(7):
                m_copy(q, tp, slot, partner).wait_send()
            for k in (1, 2, 3):
                z_ship(k, q).wait_send()
            for k in range(4):
                needed, copy = across(q, k)

                @pl.when(needed)
                def _():
                    copy.wait_send()

            for d in (1, 2, 3):
                beside(q, lax.rem(sp + d, groups), c).wait_send()

        for t in (0, 1):

            def sent(slot):
                pass_on(t, sp, tp, slot, partner).wait_send()

            pl.loop(0, 13)(sent)
            pl.loop(15, 27)(sent)
            if t:
                pass_half(sp, tp, 0, 31, partner).wait_send()
                pass_half(sp, tp, 0, 32, partner).wait_send()
                sent(35)
            else:
                pl.loop(31, 35)(sent)

            @pl.when(inner)
            def _():
                sent(13)
                pl.loop(28, 31)(sent)
                if t:
                    pl.loop(36, 40)(sent)

        for slot in (0, 1):
            for j in (0, 1):
                weight_copy(j, slot, slot).wait()
        for part in range(parts):
            down_copy(part).wait()
        for copy in finals:
            copy.wait()

    block_shape = (layers, tokens, width)
    shapes = [
        jax.ShapeDtypeStruct((parts, width, hidden), jnp.bfloat16),
        jax.ShapeDtypeStruct((parts, width, hidden), jnp.bfloat16),
        jax.ShapeDtypeStruct((hidden, parts * width), jnp.bfloat16),
    ]
    shapes += [jax.ShapeDtypeStruct((tokens, width), jnp.bfloat16)] * 3
    shapes.append(jax.ShapeDtypeStruct((2 * width, width), jnp.float32))
    half = jnp.bfloat16
    return pl.pallas_call(
        kernel,
        out_shape=shapes,
        in_specs=[pl.BlockSpec(memory_space=pl.ANY)] * 9
        + [pl.BlockSpec(memory_space=pltpu.VMEM), pl.BlockSpec(memory_space=pl.ANY)],
        out_specs=[pl.BlockSpec(memory_space=pl.ANY)] * 7,
        scratch_shapes=[
            pltpu.VMEM((2, parts, rows_all, width), half),
            pltpu.VMEM((parts, width, 2 * hidden), half),
            pltpu.VMEM((parts, hidden, width), half),
            pltpu.VMEM((layers, width, 2 * hidden), half),
            pltpu.VMEM((rows_all, 2 * hidden), jnp.float32),
            pltpu.VMEM((rows_all, hidden), jnp.float32),
            pltpu.VMEM((rows_all, 2 * hidden), half),
            pltpu.VMEM((rows_all, 2 * hidden), half),
            pltpu.VMEM((hidden, rows_all), half),
            pltpu.VMEM((2, 2, width, hidden), half),
            pltpu.VMEM((groups, 8, tokens), jnp.float32),
            pltpu.VMEM(block_shape, jnp.float32),
        ]
        + [pltpu.VMEM(block_shape, half)] * 7
        + [
            pltpu.VMEM((6, tokens, width), half),
            pltpu.VMEM((parts, width, width), half),
            pltpu.VMEM((parts, tokens, width), half),
            pltpu.VMEM((groups, 2, tokens, width), half),
            pltpu.VMEM((groups, tokens, width), half),
            pltpu.VMEM((tokens + 16, width), jnp.float32),
            pltpu.VMEM((tokens + 16, width), jnp.float32),
            pltpu.VMEM((tokens, width), jnp.float32),
            pltpu.VMEM((tokens, width), jnp.float32),
            pltpu.VMEM((3, tokens, width), half),
            pltpu.VMEM((3, tokens, width), half),
            pltpu.SemaphoreType.DMA((9 + parts,)),
            pltpu.SemaphoreType.DMA((2, 40)),
            pltpu.SemaphoreType.DMA((2, groups, parts)),
            pltpu.SemaphoreType.DMA((3,)),
            pltpu.SemaphoreType.DMA((3,)),
            pltpu.SemaphoreType.DMA((layers,)),
            pltpu.SemaphoreType.DMA((layers,)),
            pltpu.SemaphoreType.DMA((groups,)),
            pltpu.SemaphoreType.DMA((groups,)),
            pltpu.SemaphoreType.DMA((3, layers, 4)),
            pltpu.SemaphoreType.DMA((3, layers, 4)),
            pltpu.SemaphoreType.DMA((layers, 4)),
            pltpu.SemaphoreType.DMA((6, 4)),
            pltpu.SemaphoreType.DMA((8,)),
            pltpu.SemaphoreType.DMA((2, 2)),
            pltpu.SemaphoreType.DMA((parts,)),
            pltpu.SemaphoreType.DMA((2, 2)),
            pltpu.SemaphoreType.DMA((2, 2)),
            pltpu.SemaphoreType.DMA((3,)),
            pltpu.SemaphoreType.DMA((groups,)),
            pltpu.SemaphoreType.DMA((4, 7)),
            pltpu.SemaphoreType.DMA((4, parts)),
            pltpu.SemaphoreType.DMA((4, layers)),
            pltpu.SemaphoreType.DMA((4, groups)),
            pltpu.SemaphoreType.DMA((4, groups)),
            pltpu.SemaphoreType.DMA((4, groups)),
        ],
        compiler_params=pltpu.CompilerParams(
            collective_id=10, has_side_effects=True, vmem_limit_bytes=62 * 1024 * 1024
        ),
    )


def finish(grads, rest):
    pieces = 4
    count, total = (len(grads), len(grads) + len(rest))

    def kernel(*refs):
        sources, targets = (refs[:total], refs[total : 2 * total])
        narrow, broad = (refs[2 * total : 2 * total + count], refs[2 * total + count : 2 * total + 2 * count])
        through = refs[2 * total + 2 * count : 3 * total + count]
        in_sem, out_sem = refs[-2:]

        def piece(ref, i):
            size = ref.shape[0] // pieces
            return ref.at[pl.ds(i * size, size)]

        fetches = {}
        for i in range(pieces):
            for j in range(count):
                fetches[i, j] = pltpu.make_async_copy(
                    piece(sources[j], i), piece(narrow[j], i), in_sem.at[j, i]
                )
                fetches[i, j].start()
        for j in range(count, total):
            fetches[0, j] = pltpu.make_async_copy(sources[j], through[j - count], in_sem.at[j, 0])
            fetches[0, j].start()
        stores = []

        def store(source, target, j, i):
            copy = pltpu.make_async_copy(source, target, out_sem.at[j, i])
            copy.start()
            stores.append(copy)

        for i in range(pieces):
            for j in range(count):
                fetches[i, j].wait()
                size = narrow[j].shape[0] // pieces
                steps = 4
                rows = size // steps

                @pl.loop(0, steps)
                def _(n):
                    here = pl.ds(pl.multiple_of(i * size + n * rows, rows), rows)
                    broad[j][here, :] = narrow[j][here, :].astype(jnp.float32)

                store(piece(broad[j], i), piece(targets[j], i), j, i)
        for j in range(count, total):
            fetches[0, j].wait()
            store(through[j - count], targets[j], j, 0)
        for copy in stores:
            copy.wait()

    shapes = [jax.ShapeDtypeStruct(g.shape, jnp.float32) for g in grads]
    shapes += [jax.ShapeDtypeStruct(r.shape, r.dtype) for r in rest]
    return pl.pallas_call(
        kernel,
        out_shape=shapes,
        in_specs=[pl.BlockSpec(memory_space=pl.ANY)] * total,
        out_specs=[pl.BlockSpec(memory_space=pl.ANY)] * total,
        scratch_shapes=[pltpu.VMEM(g.shape, g.dtype) for g in grads]
        + [pltpu.VMEM(g.shape, jnp.float32) for g in grads]
        + [pltpu.VMEM(r.shape, r.dtype) for r in rest]
        + [pltpu.SemaphoreType.DMA((total, pieces))] * 2,
        compiler_params=pltpu.CompilerParams(vmem_limit_bytes=62 * 1024 * 1024),
    )(*grads, *rest)


def near_body(
    moe_input,
    out_gate,
    in_gate,
    values,
    conv_taps,
    out_proj,
    route_ids,
    route_gates,
    expert_gate,
    expert_up,
    expert_down,
    cotangent,
):
    token_count, part_width = moe_input.shape
    group_count = lax.axis_size("sp")
    hidden = expert_gate.shape[2]
    part_count = lax.axis_size("tp")
    chosen = route_ids[None, :, :] == jnp.arange(group_count, dtype=jnp.int32)[:, None, None]
    weights = jnp.sum(jnp.where(chosen, route_gates[None, :, :], 0.0), axis=2)
    route = jnp.broadcast_to(weights[:, None, :], (group_count, 8, token_count))
    (
        grad_expert_gate,
        grad_expert_up,
        grad_expert_down,
        grad_out_gate,
        grad_in_gate,
        grad_values,
        grad_out_proj,
    ) = experts_kernel(token_count, part_width, hidden)(
        moe_input,
        cotangent,
        route,
        expert_gate.reshape(part_count, part_width, hidden),
        expert_up.reshape(part_count, part_width, hidden),
        expert_down[0],
        out_gate,
        in_gate,
        values,
        conv_taps,
        out_proj.reshape(part_count, part_width, part_width),
    )

    (
        grad_expert_gate,
        grad_expert_up,
        grad_expert_down,
        grad_out_gate,
        grad_in_gate,
        grad_values,
        grad_out_proj,
    ) = finish(
        (
            grad_expert_gate.reshape(-1, hidden),
            grad_expert_up.reshape(-1, hidden),
            grad_expert_down,
        ),
        (grad_out_gate, grad_in_gate, grad_values, grad_out_proj),
    )
    grad_expert_gate = grad_expert_gate[None]
    grad_expert_up = grad_expert_up[None]
    grad_expert_down = grad_expert_down[None]
    return (
        grad_out_gate,
        grad_in_gate,
        grad_values,
        grad_out_proj,
        grad_expert_gate,
        grad_expert_up,
        grad_expert_down,
    )


def step(*arrays):
    moe_input, expert_gate, out_proj = (arrays[0], arrays[8], arrays[5])
    tokens, width = moe_input.shape
    near = (
        lax.axis_size("sp") == 4
        and lax.axis_size("tp") == 8
        and expert_gate.shape[0] == 1
        and tokens % 256 == 0
        and width == 2 * expert_gate.shape[2] == 2 * tokens
        and out_proj.shape[0] == 8 * width
    )
    return (near_body if near else body)(*arrays)


def solution(mesh):
    return jax.shard_map(
        step,
        mesh=mesh,
        in_specs=(
            P("sp", "tp"),
            P("sp", "tp"),
            P("sp", "tp"),
            P("sp", "tp"),
            P(None, "tp"),
            P(None, "tp"),
            P("sp", None),
            P("sp", None),
            P("sp", None, "tp"),
            P("sp", None, "tp"),
            P("sp", "tp", None),
            P("sp", "tp"),
        ),
        out_specs=(
            P("sp", "tp"),
            P("sp", "tp"),
            P("sp", "tp"),
            P("sp", "tp"),
            P("sp", None, "tp"),
            P("sp", None, "tp"),
            P("sp", "tp", None),
        ),
        check_vma=False,
    )
```
